512 devices in a mesh: ep: 32 (over z, core), tp: 16 (over y, x).
Axes of the slice: x: 4, y: 4, z: 16, core: 2. Of those that a mesh axis runs over, the one named last changes fastest.
Arguments:
- tokens: bfloat16 [512, 2048], P('ep'), may hold values from -6 to 6
- mix_gain: float32 [2048], replicated, may hold values from 0.1 to 1.9
- gate_weight: bfloat16 [2048, 1024], P('ep', 'tp'), may hold values from -0.125 to 0.125
- inner_weight: bfloat16 [2048, 1024], P('ep', 'tp'), may hold values from -0.125 to 0.125
- write_weight: bfloat16 [2048, 512], P('ep'), may hold values from -0.125 to 0.125
- read_weight: bfloat16 [2048, 512], P('ep'), may hold values from -0.125 to 0.125
- step_weight: bfloat16 [2048, 16], P('ep'), may hold values from -0.125 to 0.125
- step_bias: float32 [16], replicated, may hold values from -2 to 1
- decay_log: float32 [16], replicated, may hold values from -1 to 1.5
- skip_scale: float32 [16], replicated, may hold values from 0.5 to 2
- inner_taps: bfloat16 [4, 1024], P(None, 'tp'), may hold values from -3 to 3
- access_taps: bfloat16 [2, 4, 512], replicated, may hold values from -3 to 3
- inner_history: bfloat16 [512, 3, 1024], P('ep', None, 'tp'), may hold values from -6 to 6
- access_history: bfloat16 [512, 2, 3, 512], P('ep'), may hold values from -6 to 6
- recurrent: float32 [512, 16, 64, 128], P('ep', 'tp'), may hold values from -3 to 3
- head_gain: float32 [1024], P('tp'), may hold values from 0.1 to 1.9
- mixer_out: bfloat16 [1024, 2048], P('tp'), may hold values from -0.1875 to 0.1875
- moe_gain: float32 [2048], replicated, may hold values from 0.1 to 1.9
- expert_ids: int32 [512, 2], P('ep'), may hold values from 0 to 31, all different within a row; in each aligned block of 16 rows (0 to 15, 16 to 31, ...) at most 2 rows name the same one
- route_scores: float32 [512, 2], P('ep'), may hold values from -6 to 6
- expert_gate: bfloat16 [32, 2048, 4096], P('ep', None, 'tp'), may hold values from -0.125 to 0.125
- expert_up: bfloat16 [32, 2048, 4096], P('ep', None, 'tp'), may hold values from -0.125 to 0.125
- expert_down: bfloat16 [32, 4096, 2048], P('ep', 'tp'), may hold values from -0.1875 to 0.1875
- blend_vector: bfloat16 [2048], replicated, may hold values from -0.125 to 0.125
- dense_gate: bfloat16 [2048, 7168], P('tp', 'ep'), may hold values from -0.125 to 0.125
- dense_up: bfloat16 [2048, 7168], P('tp', 'ep'), may hold values from -0.125 to 0.125
- dense_down: bfloat16 [7168, 2048], P('ep', 'tp'), may hold values from -0.125 to 0.125
Outputs:
- output: float32 [512, 2048], P('ep', 'tp')
- new_recurrent: float32 [512, 16, 64, 128], P('ep', 'tp')
- new_inner_history: bfloat16 [512, 3, 1024], P('ep', None, 'tp')
- new_access_history: bfloat16 [512, 2, 3, 512], P('ep')
The draws below stay inside these ranges and needn't reach their ends.
Inputs may be any that keep to these rules, and one draw needn't show every extreme that they name: `expert_ids`: each row names 2 different experts; among the rows of one device no expert is named by more than 2 rows, and in some aligned blocks of 16 rows one expert is named by exactly 2.
All inputs are finite; a program needn't handle non-finite values.
Results may differ from the reference program's by a relative error of at most 0.009.
Values may be sent and summed in bfloat16 or wider, within the bound.
No kernel may reach another device: no remote copies, remote signals or barrier semaphores. Data moves between devices by JAX's collectives and lax.ppermute only.
A program may use at most 64 MiB of HBM per device.

```python
import math
import jax
import jax.numpy as jnp
import numpy as np
from jax import lax

D = 2048
HEADS = 16
HEAD_DIM = 64
GROUPS = 4
STATE = 128
TAPS = 4
FF = 4096
DF = 7168
TOP = 2
SEQS = 16
INNER = 1024
EXPERTS = 32
CAP = 2
TOKENS = 512
N_EP = 32


def levels(own_key, extent, split, smallest, largest):
    factor_of, own = 1.0, jax.random.fold_in(own_key, 6)
    for position, parts in split:
        heights = jnp.exp(jax.random.uniform(jax.random.fold_in(own, position), (parts,), jnp.float32, smallest / len(split), largest / len(split)))
        factor_of = factor_of * jnp.repeat(heights, extent[position] // parts).reshape([-1 if axis == position else 1 for axis in range(len(extent))])
    return factor_of


def routed_block(rng, own, number, rows, count, top, bound, skew):
    sequence = jax.random.permutation(rng, count)
    crowded, usual = shares(count, rows * top, bound, skew, True), shares(count, rows * top, bound, skew, False)
    places = jnp.arange(count)

    def named(sizes, rotation):
        used = int((sizes > 0).sum())
        fixed = max(1, used // 4)
        moved = fixed + (places - fixed + rotation * (used - fixed)) % max(1, count - fixed)
        return jnp.zeros((count,), jnp.int32).at[sequence[jnp.where(places < fixed, places, moved)]].set(jnp.asarray(sizes, jnp.int32))

    sizes = jnp.where(number % 4 == 0, named(crowded, number // 4), named(usual, number - number // 4 - 1))
    mixed = jax.random.permutation(jax.random.fold_in(own, 3), count)
    source_of, receiver = mixed[0:count // 2 * 2:2], mixed[1:count // 2 * 2:2]
    room = jnp.minimum(sizes[source_of] - 1, bound - sizes[receiver]) // 2
    room = jnp.where((source_of == sequence[0]) | (receiver == sequence[0]) | (sizes[receiver] == 0), 0, jnp.maximum(room, 0))
    moved = jax.random.randint(jax.random.fold_in(own, 4), (count // 2,), 0, 1 << 20) % (room + 1)
    sizes = sizes.at[source_of].add(-moved).at[receiver].add(moved)
    items = jnp.searchsorted(jnp.cumsum(sizes), jnp.arange(rows * top), side="right").astype(jnp.int32)
    table = items.reshape(top, rows).T
    table = table[jax.random.permutation(jax.random.fold_in(own, 1), rows)]
    rotation = jax.random.randint(jax.random.fold_in(own, 2), (rows, 1), 0, top)
    return jnp.take_along_axis(table, (jnp.arange(top)[None, :] + rotation) % top, axis=1)


def shares(number_of, total, limit, slope, full):
    loads = [(1 << 20) // math.isqrt(standing ** slope) + 1 for standing in range(1, number_of + 1)]
    largest = limit if full else min(limit, max(-(-total // number_of), total * loads[0] // sum(loads)))
    least = 1 if total - largest >= number_of - 1 else 0
    given, rest = [largest] + [least] * (number_of - 1), total - largest - least * (number_of - 1)
    while rest > 0:
        movable = [i for i in range(1, number_of) if given[i] < largest] or [i for i in range(1, number_of) if given[i] < limit]
        pool, remaining = sum([loads[i] for i in movable]), rest
        for i in movable:
            addition = min(limit - given[i], max(1, remaining * loads[i] // pool), rest)
            given[i] = given[i] + addition
            rest = rest - addition
    return np.array(given)


def scatter_about(rng, shape, deviation, bound, shards=(), dtype=jnp.bfloat16):
    array = jax.random.normal(rng, shape, jnp.float32) * deviation
    if len(shards) > 0:
        array = levels(rng, shape, shards, -0.22, 0.18) * array
    return jnp.clip(array, min=-bound, max=bound).astype(dtype)


def setup_inputs(seed: int = 0) -> dict:
    key_of = jax.random.split(jax.random.key(seed), 28)
    tokens = scatter_about(key_of[0], (TOKENS, D), 1.0, 6.0, ((0, 32),))
    mix_gain = jnp.clip(1.0 + 0.18 * jax.random.normal(key_of[1], (D,), jnp.float32), 0.1, 1.9)
    gate_weight = scatter_about(key_of[2], (D, INNER), D ** -0.5, 0.125, ((0, 32), (1, 16)))
    inner_weight = scatter_about(key_of[3], (D, INNER), D ** -0.5, 0.125, ((0, 32), (1, 16)))
    write_weight = scatter_about(key_of[4], (D, GROUPS * STATE), D ** -0.5, 0.125, ((0, 32),))
    read_weight = scatter_about(key_of[5], (D, GROUPS * STATE), D ** -0.5, 0.125, ((0, 32),))
    step_weight = scatter_about(key_of[6], (D, HEADS), D ** -0.5, 0.125, ((0, 32),))
    step_bias = jnp.clip(jax.random.uniform(key_of[7], (HEADS,), jnp.float32, -2.0, 1.0), -2.0, 1.0)
    decay_log = jnp.clip(jax.random.uniform(key_of[8], (HEADS,), jnp.float32, -1.0, 1.5), -1.0, 1.5)
    skip_scale = jnp.clip(jax.random.uniform(key_of[9], (HEADS,), jnp.float32, 0.5, 2.0), 0.5, 2.0)
    inner_taps = scatter_about(key_of[10], (TAPS, INNER), 0.5, 3.0, ((1, 16),))
    access_taps = scatter_about(key_of[11], (2, TAPS, GROUPS * STATE), 0.5, 3.0)
    inner_history = scatter_about(key_of[12], (TOKENS, TAPS - 1, INNER), 1.0, 6.0, ((0, 32), (2, 16)))
    access_history = scatter_about(key_of[13], (TOKENS, 2, TAPS - 1, GROUPS * STATE), 1.0, 6.0, ((0, 32),))
    recurrent = scatter_about(key_of[14], (TOKENS, HEADS, HEAD_DIM, STATE), 0.5, 3.0, ((0, 32), (1, 16)), jnp.float32)
    head_gain = jnp.clip(1.0 + 0.18 * jax.random.normal(key_of[15], (INNER,), jnp.float32), 0.1, 1.9)
    mixer_out = scatter_about(key_of[16], (INNER, D), INNER ** -0.5, 0.1875, ((0, 16),))
    moe_gain = jnp.clip(1.0 + 0.18 * jax.random.normal(key_of[17], (D,), jnp.float32), 0.1, 1.9)
    expert_ids_keys = jax.random.split(jax.random.fold_in(key_of[18], 1), TOKENS // SEQS)
    expert_ids_turns = jax.random.permutation(jax.random.fold_in(key_of[18], 3), TOKENS // SEQS)
    expert_ids = jax.vmap(lambda own, number: routed_block(jax.random.fold_in(key_of[18], 2), own, number, SEQS, EXPERTS, TOP, CAP, 2))(expert_ids_keys, expert_ids_turns).reshape((TOKENS, TOP))
    route_scores = scatter_about(key_of[19], (TOKENS, TOP), 1.0, 6.0, ((0, 32),), jnp.float32)
    expert_gate = scatter_about(key_of[20], (EXPERTS, D, FF), D ** -0.5, 0.125, ((0, 32), (2, 16)))
    expert_up = scatter_about(key_of[21], (EXPERTS, D, FF), D ** -0.5, 0.125, ((0, 32), (2, 16)))
    expert_down = scatter_about(key_of[22], (EXPERTS, FF, D), (FF // 4) ** -0.5, 0.1875, ((0, 32), (1, 16)))
    blend_vector = scatter_about(key_of[23], (D,), D ** -0.5, 0.125)
    dense_gate = scatter_about(key_of[24], (D, DF), D ** -0.5, 0.125, ((0, 16), (1, 32)))
    dense_up = scatter_about(key_of[25], (D, DF), D ** -0.5, 0.125, ((0, 16), (1, 32)))
    dense_down = scatter_about(key_of[26], (DF, D), (DF // 4) ** -0.5, 0.125, ((0, 32), (1, 16)))
    return dict(tokens=tokens, mix_gain=mix_gain, gate_weight=gate_weight, inner_weight=inner_weight, write_weight=write_weight, read_weight=read_weight, step_weight=step_weight, step_bias=step_bias, decay_log=decay_log, skip_scale=skip_scale, inner_taps=inner_taps, access_taps=access_taps, inner_history=inner_history, access_history=access_history, recurrent=recurrent, head_gain=head_gain, mixer_out=mixer_out, moe_gain=moe_gain, expert_ids=expert_ids, route_scores=route_scores, expert_gate=expert_gate, expert_up=expert_up, expert_down=expert_down, blend_vector=blend_vector, dense_gate=dense_gate, dense_up=dense_up, dense_down=dense_down)


EPS = 1e-06

def rms_scale(values, gain):
    mean_square = lax.optimization_barrier(jnp.mean(values * values, axis=-1, keepdims=True))
    return values * lax.rsqrt(mean_square + EPS) * gain

def reference(tokens, mix_gain, gate_weight, inner_weight, write_weight, read_weight, step_weight, step_bias, decay_log, skip_scale, inner_taps, access_taps, inner_history, access_history, recurrent, head_gain, mixer_out, moe_gain, expert_ids, route_scores, expert_gate, expert_up, expert_down, blend_vector, dense_gate, dense_up, dense_down):
    count = tokens.shape[0]
    normed = rms_scale(tokens.astype(jnp.float32), mix_gain).astype(jnp.bfloat16)
    gate_part = jnp.dot(normed, gate_weight, preferred_element_type=jnp.float32).astype(jnp.bfloat16)
    inner_part = jnp.dot(normed, inner_weight, preferred_element_type=jnp.float32).astype(jnp.bfloat16)
    write_part = jnp.dot(normed, write_weight, preferred_element_type=jnp.float32).astype(jnp.bfloat16)
    read_part = jnp.dot(normed, read_weight, preferred_element_type=jnp.float32).astype(jnp.bfloat16)
    step_raw = jnp.dot(normed, step_weight, preferred_element_type=jnp.float32)
    inner_window = jnp.concatenate([inner_history, inner_part[:, None, :]], axis=1)
    inner_conv = jax.nn.silu(lax.optimization_barrier(jnp.sum(inner_window.astype(jnp.float32) * inner_taps.astype(jnp.float32)[None], axis=1)))
    access_window = jnp.concatenate([access_history, jnp.stack([write_part, read_part], axis=1)[:, :, None, :]], axis=2)
    access_conv = jax.nn.silu(lax.optimization_barrier(jnp.sum(access_window.astype(jnp.float32) * access_taps.astype(jnp.float32)[None], axis=2)))
    per_group = HEADS // GROUPS
    write_heads = jnp.repeat(access_conv[:, 0].reshape(count, GROUPS, STATE), per_group, axis=1)
    read_heads = jnp.repeat(access_conv[:, 1].reshape(count, GROUPS, STATE), per_group, axis=1)
    step = jax.nn.softplus(step_raw + step_bias[None, :])
    decay = jnp.exp(-step * jnp.exp(decay_log)[None, :])
    inner_heads = inner_conv.reshape(count, HEADS, HEAD_DIM)
    new_recurrent = decay[:, :, None, None] * recurrent + (step[:, :, None] * inner_heads)[..., None] * write_heads[:, :, None, :]
    readout = lax.optimization_barrier(jnp.sum(new_recurrent * read_heads[:, :, None, :], axis=-1)) + skip_scale[None, :, None] * inner_heads
    gated = readout * jax.nn.silu(gate_part.astype(jnp.float32).reshape(count, HEADS, HEAD_DIM))
    head_out = rms_scale(gated, head_gain.reshape(HEADS, HEAD_DIM)).reshape(count, HEADS * HEAD_DIM).astype(jnp.bfloat16)
    mixed = jnp.dot(head_out, mixer_out, preferred_element_type=jnp.float32).astype(jnp.bfloat16)
    resid = tokens.astype(jnp.float32) + mixed.astype(jnp.float32)
    hidden = rms_scale(resid, moe_gain).astype(jnp.bfloat16)
    first = jax.nn.sigmoid(route_scores[:, 0] - route_scores[:, 1])
    weights = jnp.stack([first, 1.0 - first], axis=1).reshape(-1)
    flat_ids = expert_ids.reshape(-1)
    flat_token = (jnp.arange(count * TOP) // TOP).astype(jnp.int32)
    most = CAP * N_EP

    def one_expert(total, expert):
        chosen = flat_ids == expert
        picked = jnp.nonzero(chosen, size=most, fill_value=0)[0].astype(jnp.int32)
        valid = (jnp.arange(most) < jnp.sum(chosen.astype(jnp.int32))).astype(jnp.float32)
        rows = hidden[flat_token[picked]]
        gate_vals = jnp.dot(rows, expert_gate[expert], preferred_element_type=jnp.float32)
        up_vals = jnp.dot(rows, expert_up[expert], preferred_element_type=jnp.float32)
        act = (jax.nn.silu(gate_vals) * up_vals).astype(jnp.bfloat16)
        expert_out = jnp.dot(act, expert_down[expert], preferred_element_type=jnp.float32).astype(jnp.bfloat16)
        share = expert_out.astype(jnp.float32) * (weights[picked] * valid)[:, None]
        return (total.at[flat_token[picked]].add(share), None)
    routed, unused = lax.scan(one_expert, jnp.zeros((count, tokens.shape[1]), jnp.float32), jnp.arange(EXPERTS).astype(jnp.int32))
    dense_g = jnp.dot(hidden, dense_gate, preferred_element_type=jnp.float32)
    dense_u = jnp.dot(hidden, dense_up, preferred_element_type=jnp.float32)
    dense_act = (jax.nn.silu(dense_g) * dense_u).astype(jnp.bfloat16)
    dense_out = jnp.dot(dense_act, dense_down, preferred_element_type=jnp.float32)
    blend = jax.nn.sigmoid(jnp.dot(hidden, blend_vector, preferred_element_type=jnp.float32))
    output = resid + routed + blend[:, None] * dense_out
    return (output, new_recurrent, inner_window[:, 1:], access_window[:, :, 1:])
```

```python
import jax
import jax.numpy as jnp
from jax import lax
from jax.sharding import PartitionSpec as P

HEADS = 16
HEAD_DIM = 64
GROUPS = 4
STATE = 128
TOP = 2
PER_GROUP = HEADS // GROUPS
EPS = 1e-06
BF = jnp.bfloat16
F32 = jnp.float32
CORES = 2


def exchange(pieces, axis, groups=None):
    return lax.all_to_all(
        pieces, axis, split_axis=0, concat_axis=0, tiled=True, axis_index_groups=groups
    )


def to_everyone(shard, peers):
    return jnp.broadcast_to(shard[None], (peers, *shard.shape))


def rms_scale(values, gain):
    mean_square = jnp.mean(values * values, axis=-1, keepdims=True)
    return values * lax.rsqrt(mean_square + EPS) * gain


def dot32(left, right):
    return jnp.dot(left, right, preferred_element_type=F32)


def slice_at(array, start, size, dim):
    return lax.dynamic_slice_in_dim(array, start, size, dim)


def local(
    tokens,
    mix_gain,
    gate_weight,
    inner_weight,
    write_weight,
    read_weight,
    step_weight,
    step_bias,
    decay_log,
    skip_scale,
    inner_taps,
    access_taps,
    inner_history,
    access_history,
    recurrent,
    head_gain,
    mixer_out,
    moe_gain,
    expert_ids,
    route_scores,
    expert_gate,
    expert_up,
    expert_down,
    blend_vector,
    dense_gate,
    dense_up,
    dense_down,
):
    seqs, width = tokens.shape
    n_ep = lax.axis_size("ep")
    n_tp = lax.axis_size("tp")
    chips = n_ep // CORES
    ep = lax.axis_index("ep")
    tp = lax.axis_index("tp")
    core = ep % CORES
    group = tp // PER_GROUP
    rows_k = gate_weight.shape[0]
    cols = width // n_tp
    same_core = [[CORES * z + c for z in range(chips)] for c in range(CORES)]
    swap = [(i, i ^ 1) for i in range(n_ep)]

    write_own = slice_at(write_weight, group * STATE, STATE, 1)
    read_own = slice_at(read_weight, group * STATE, STATE, 1)
    main = jnp.concatenate([gate_weight, inner_weight, write_own, read_own], axis=1)
    pack_cols = main.shape[1]
    head_pick = (jnp.arange(HEADS) == tp).astype(BF)[None]
    step_row = lax.dot_general(
        head_pick, step_weight, (((1,), (1,)), ((), ())), preferred_element_type=F32
    ).astype(BF)
    first = jax.nn.sigmoid(route_scores[:, 0] - route_scores[:, 1])
    first_high = first.astype(BF).astype(F32)
    first_low = first - first_high
    lane = jnp.arange(4 * seqs)[None]
    spread = jnp.where(
        lane < seqs,
        expert_ids[:, 0:1].astype(F32),
        jnp.where(
            lane < 2 * seqs,
            expert_ids[:, 1:2].astype(F32),
            jnp.where(lane < 3 * seqs, first_high[:, None], first_low[:, None]),
        ),
    )
    route_row = jnp.sum(
        jnp.where(lane % seqs == jnp.arange(seqs)[:, None], spread, 0.0), axis=0, keepdims=True
    ).astype(BF)
    extra = jnp.concatenate([step_row, route_row, jnp.zeros((6, rows_k), BF)], axis=0)
    extra = jnp.pad(extra, ((0, 0), (0, pack_cols - rows_k)))
    pack = jnp.concatenate([main, extra], axis=0)
    own_pack = exchange(to_everyone(pack, chips), "ep", same_core)
    other_pack = lax.ppermute(own_pack, "ep", swap)

    normed = rms_scale(tokens.astype(F32), mix_gain).astype(BF)
    by_core = normed.reshape(seqs, chips, CORES, rows_k)
    own_k = jnp.where(core == 0, by_core[:, :, 0], by_core[:, :, 1])
    other_k = jnp.where(core == 0, by_core[:, :, 1], by_core[:, :, 0])

    def projected_by(keys, packed):
        padded = jnp.pad(keys, ((0, 0), (0, 0), (0, packed.shape[1] - rows_k)))
        main_part = dot32(padded.reshape(seqs, -1), packed.reshape(-1, pack_cols))
        weights = packed[:, rows_k, :rows_k].astype(F32)
        step_part = jnp.sum(keys.astype(F32) * weights[None], axis=(1, 2))
        return main_part, step_part

    main_a, step_a = projected_by(own_k, own_pack)
    main_b, step_b = projected_by(other_k, other_pack)
    projected = main_a + main_b
    step_raw = step_a + step_b
    gate_part = projected[:, :HEAD_DIM].astype(BF)
    inner_part = projected[:, HEAD_DIM : 2 * HEAD_DIM].astype(BF)
    write_part = projected[:, 2 * HEAD_DIM : 2 * HEAD_DIM + STATE].astype(BF)
    read_part = projected[:, 2 * HEAD_DIM + STATE :].astype(BF)

    inner_window = jnp.concatenate([inner_history, inner_part[:, None, :]], axis=1)
    inner_conv = jax.nn.silu(
        jnp.sum(inner_window.astype(F32) * inner_taps.astype(F32)[None], axis=1)
    )
    history_own = slice_at(access_history, group * STATE, STATE, 3).astype(F32)
    taps_own = slice_at(access_taps, group * STATE, STATE, 2).astype(F32)

    def access_conv(which, part):
        taps = taps_own[which]
        past = jnp.sum(history_own[:, which] * taps[None, :3], axis=1)
        return jax.nn.silu(past + part.astype(F32) * taps[3][None])

    write_conv = access_conv(0, write_part)
    read_conv = access_conv(1, read_part)
    bias_own = slice_at(step_bias, tp, 1, 0)
    rate_own = slice_at(decay_log, tp, 1, 0)
    skip_own = slice_at(skip_scale, tp, 1, 0)
    step = jax.nn.softplus(step_raw + bias_own)
    decay = jnp.exp(-step * jnp.exp(rate_own))
    new_recurrent = (
        decay[:, None, None] * recurrent[:, 0]
        + (step[:, None] * inner_conv)[..., None] * write_conv[:, None, :]
    )
    readout = jnp.sum(new_recurrent * read_conv[:, None, :], axis=-1) + skip_own * inner_conv
    gated = readout * jax.nn.silu(gate_part.astype(F32))
    head_out = rms_scale(gated, head_gain).astype(BF)

    partial_mix = dot32(head_out, mixer_out)
    mix_pieces = partial_mix.reshape(seqs, n_tp, cols).transpose(1, 0, 2)
    parts_sent = jnp.where(tp % 2 == 0, write_part, read_part).astype(F32)
    arrived = exchange(
        jnp.concatenate([mix_pieces, to_everyone(parts_sent, n_tp)], axis=1), "tp"
    )
    mixed = jnp.sum(arrived[:, :seqs], axis=0).astype(BF)
    parts_all = arrived[:, seqs:].astype(BF).reshape(GROUPS, PER_GROUP, seqs, STATE)[:, :2]
    parts_all = parts_all.transpose(2, 1, 0, 3).reshape(seqs, 2, 1, GROUPS * STATE)
    new_access = jnp.concatenate([access_history[:, :, 1:], parts_all], axis=2)

    resid = slice_at(tokens, tp * cols, cols, 1).astype(F32) + mixed.astype(F32)
    gain_own = slice_at(moe_gain, tp * cols, cols, 0)
    scaled = (resid * gain_own).astype(BF)
    scaled_all = exchange(to_everyone(scaled, n_ep), "ep").reshape(n_ep * seqs, cols)

    own_routes = own_pack[:, rows_k + 1, : 4 * seqs].astype(F32)
    other_routes = other_pack[:, rows_k + 1, : 4 * seqs].astype(F32)
    routes = jnp.where(
        core == 0,
        jnp.stack([own_routes, other_routes], axis=1),
        jnp.stack([other_routes, own_routes], axis=1),
    ).reshape(n_ep, 4 * seqs)
    mine = ep.astype(F32)
    is_first = routes[:, :seqs] == mine
    is_second = routes[:, seqs : 2 * seqs] == mine
    first_all = routes[:, 2 * seqs : 3 * seqs] + routes[:, 3 * seqs :]
    weight = jnp.where(is_first, first_all, 1.0 - first_all)
    named = is_first | is_second
    earlier = (jnp.arange(seqs)[:, None] < jnp.arange(seqs)[None]).astype(BF)
    rank = dot32(named.astype(BF), earlier)
    key = jnp.where(named, rank, -1.0)
    total = n_ep * seqs
    place = jnp.arange(total)[None]
    tiled = (place % seqs == jnp.arange(seqs)[:, None]).astype(F32)
    own_block = place // seqs == jnp.arange(n_ep)[:, None]
    spread = jnp.dot(
        jnp.concatenate([key, weight], axis=0), tiled, precision=lax.Precision.HIGHEST
    )
    key_row = jnp.sum(jnp.where(own_block, spread[:n_ep], 0.0), axis=0, keepdims=True)
    weight_row = jnp.sum(jnp.where(own_block, spread[n_ep:], 0.0), axis=0, keepdims=True)
    slots = TOP * n_ep
    slot = jnp.arange(slots)[:, None]
    chosen = (slot // TOP == place // seqs) & (key_row == (slot % TOP).astype(F32))
    slot_weight = jnp.sum(jnp.where(chosen, weight_row, 0.0), axis=1, keepdims=True)
    chosen = chosen.astype(BF)

    units = dense_gate.shape[1]
    half = -(-(units + 2) // 128) * 128
    blend_col = slice_at(blend_vector, tp * cols, cols, 0)[:, None]
    both_dense = jnp.concatenate(
        [
            dense_gate,
            blend_col,
            jnp.zeros((cols, half - units - 1), BF),
            dense_up,
            jnp.zeros((cols, half - units), BF),
        ],
        axis=1,
    )
    plain = scaled_all.astype(F32) / gain_own
    square_sum = jnp.sum(plain * plain, axis=1, keepdims=True)
    dense_partial = dot32(scaled_all, both_dense)
    dense_partial = jnp.where(
        jnp.arange(2 * half)[None] == units + 1, square_sum, dense_partial
    ).astype(BF)
    expert_rows = dot32(chosen, scaled_all).astype(BF)
    quarter = slots * cols // (2 * half)
    expert_block = (
        expert_rows.reshape(slots // quarter, quarter, cols)
        .transpose(1, 0, 2)
        .reshape(quarter, 2 * half)
    )
    share = total // n_tp
    arrived = exchange(
        jnp.concatenate(
            [dense_partial.reshape(n_tp, share, 2 * half), to_everyone(expert_block, n_tp)],
            axis=1,
        ),
        "tp",
    )
    dense_inner = jnp.sum(arrived[:, :share].astype(F32), axis=0)
    rows = (
        arrived[:, share:]
        .reshape(n_tp, quarter, slots // quarter, cols)
        .transpose(2, 1, 0, 3)
        .reshape(slots, width)
    )
    plain_rows = rows.astype(F32) / moe_gain
    row_scale = lax.rsqrt(jnp.mean(plain_rows * plain_rows, axis=1, keepdims=True) + EPS)
    gate_vals = dot32(rows, expert_gate[0]) * row_scale
    up_vals = dot32(rows, expert_up[0]) * row_scale
    act = (jax.nn.silu(gate_vals) * up_vals).astype(BF)
    partial_out = dot32(act, expert_down[0]).astype(BF)
    out_pieces = partial_out.reshape(slots, n_tp, cols).transpose(1, 0, 2)
    scale = lax.rsqrt(dense_inner[:, units + 1 : units + 2] / width + EPS)
    blend = jax.nn.sigmoid(dense_inner[:, units : units + 1] * scale)
    dense_act = (
        blend * jax.nn.silu(dense_inner[:, :half] * scale) * (dense_inner[:, half:] * scale)
    ).astype(BF)
    act_block = jnp.concatenate([dense_act[:, :128], dense_act[:, 128:]], axis=0)
    arrived = exchange(
        jnp.concatenate([out_pieces, to_everyone(act_block, n_tp)], axis=1), "tp"
    )
    expert_out = jnp.sum(arrived[:, :slots].astype(F32), axis=0) * slot_weight
    down = jnp.pad(dense_down, ((0, half - units), (0, 0)))
    summed = (
        dot32(arrived[:, slots : slots + share].reshape(total, 128), down[:128])
        + dot32(arrived[:, slots + share :].reshape(total, 128), down[128:])
        + lax.dot_general(
            chosen, expert_out.astype(BF), (((0,), (0,)), ((), ())), preferred_element_type=F32
        )
    )
    final = exchange(summed.astype(BF).reshape(n_ep, seqs, cols), "ep")
    output = resid + jnp.sum(final.astype(F32), axis=0)
    return (output, new_recurrent[:, None], inner_window[:, 1:], new_access)


def solution(mesh):
    in_specs = (
        P("ep", None),
        P(),
        P("ep", "tp"),
        P("ep", "tp"),
        P("ep", None),
        P("ep", None),
        P("ep", None),
        P(),
        P(),
        P(),
        P(None, "tp"),
        P(),
        P("ep", None, "tp"),
        P("ep", None, None, None),
        P("ep", "tp", None, None),
        P("tp"),
        P("tp", None),
        P(),
        P("ep", None),
        P("ep", None),
        P("ep", None, "tp"),
        P("ep", None, "tp"),
        P("ep", "tp", None),
        P(),
        P("tp", "ep"),
        P("tp", "ep"),
        P("ep", "tp"),
    )
    out_specs = (
        P("ep", "tp"),
        P("ep", "tp", None, None),
        P("ep", None, "tp"),
        P("ep", None, None, None),
    )
    return jax.shard_map(local, mesh=mesh, in_specs=in_specs, out_specs=out_specs, check_vma=False)
```

```python
import jax
import jax.numpy as jnp
from jax import lax
from jax.sharding import PartitionSpec as P

HEADS = 16
HEAD_DIM = 64
GROUPS = 4
STATE = 128
TOP = 2
PER_GROUP = HEADS // GROUPS
EPS = 1e-06
BF = jnp.bfloat16
F32 = jnp.float32
CORES = 2


def exchange(pieces, axis, groups=None):
    return lax.all_to_all(
        pieces, axis, split_axis=0, concat_axis=0, tiled=True, axis_index_groups=groups
    )


def to_everyone(shard, peers):
    return jnp.broadcast_to(shard[None], (peers, *shard.shape))


def rms_scale(values, gain):
    mean_square = jnp.mean(values * values, axis=-1, keepdims=True)
    return values * lax.rsqrt(mean_square + EPS) * gain


def dot32(left, right):
    return jnp.dot(left, right, preferred_element_type=F32)


def slice_at(array, start, size, dim):
    return lax.dynamic_slice_in_dim(array, start, size, dim)


def local(
    tokens,
    mix_gain,
    gate_weight,
    inner_weight,
    write_weight,
    read_weight,
    step_weight,
    step_bias,
    decay_log,
    skip_scale,
    inner_taps,
    access_taps,
    inner_history,
    access_history,
    recurrent,
    head_gain,
    mixer_out,
    moe_gain,
    expert_ids,
    route_scores,
    expert_gate,
    expert_up,
    expert_down,
    blend_vector,
    dense_gate,
    dense_up,
    dense_down,
):
    seqs, width = tokens.shape
    n_ep = lax.axis_size("ep")
    n_tp = lax.axis_size("tp")
    chips = n_ep // CORES
    ep = lax.axis_index("ep")
    tp = lax.axis_index("tp")
    core = ep % CORES
    group = tp // PER_GROUP
    member = tp % PER_GROUP
    rows_k = gate_weight.shape[0]
    cols = width // n_tp
    same_core = [[CORES * z + c for z in range(chips)] for c in range(CORES)]
    swap = [(i, i ^ 1) for i in range(n_ep)]
    same_group = [[PER_GROUP * g + m for m in range(PER_GROUP)] for g in range(GROUPS)]
    part = 2 * STATE // PER_GROUP

    write_own = slice_at(write_weight, group * STATE, STATE, 1)
    read_own = slice_at(read_weight, group * STATE, STATE, 1)
    either = jnp.where(member < PER_GROUP // 2, write_own, read_own)
    either = jnp.where(member % 2 == 0, either[:, :part], either[:, part:])
    main = jnp.concatenate([gate_weight, inner_weight, either], axis=1)
    pack_cols = main.shape[1]
    head_pick = (jnp.arange(HEADS) == tp).astype(BF)[None]
    step_row = lax.dot_general(
        head_pick, step_weight, (((1,), (1,)), ((), ())), preferred_element_type=F32
    ).astype(BF)
    first = jax.nn.sigmoid(route_scores[:, 0] - route_scores[:, 1])
    first_high = first.astype(BF).astype(F32)
    first_low = first - first_high
    lane = jnp.arange(4 * seqs)[None]
    spread = jnp.where(
        lane < seqs,
        expert_ids[:, 0:1].astype(F32),
        jnp.where(
            lane < 2 * seqs,
            expert_ids[:, 1:2].astype(F32),
            jnp.where(lane < 3 * seqs, first_high[:, None], first_low[:, None]),
        ),
    )
    route_row = jnp.sum(
        jnp.where(lane % seqs == jnp.arange(seqs)[:, None], spread, 0.0), axis=0, keepdims=True
    ).astype(BF)
    extra = jnp.concatenate([step_row, route_row, jnp.zeros((6, rows_k), BF)], axis=0)
    extra = jnp.pad(extra, ((0, 0), (0, pack_cols - rows_k)))
    pack = jnp.concatenate([main, extra], axis=0)
    own_pack = exchange(to_everyone(pack, chips), "ep", same_core)
    other_pack = lax.ppermute(own_pack, "ep", swap)

    normed = rms_scale(tokens.astype(F32), mix_gain).astype(BF)
    by_core = normed.reshape(seqs, chips, CORES, rows_k)
    own_k = jnp.where(core == 0, by_core[:, :, 0], by_core[:, :, 1])
    other_k = jnp.where(core == 0, by_core[:, :, 1], by_core[:, :, 0])

    def projected_by(keys, packed):
        padded = jnp.pad(keys, ((0, 0), (0, 0), (0, packed.shape[1] - rows_k)))
        main_part = dot32(padded.reshape(seqs, -1), packed.reshape(-1, pack_cols))
        weights = packed[:, rows_k, :rows_k].astype(F32)
        step_part = jnp.sum(keys.astype(F32) * weights[None], axis=(1, 2))
        return main_part, step_part

    main_a, step_a = projected_by(own_k, own_pack)
    main_b, step_b = projected_by(other_k, other_pack)
    projected = main_a + main_b
    step_raw = step_a + step_b
    gate_part = projected[:, :HEAD_DIM].astype(BF)
    inner_part = projected[:, HEAD_DIM : 2 * HEAD_DIM].astype(BF)
    share_part = projected[:, 2 * HEAD_DIM :].astype(BF)
    none = jnp.zeros_like(share_part)
    placed = jnp.where(
        member % 2 == 0,
        jnp.concatenate([share_part, none], axis=1),
        jnp.concatenate([none, share_part], axis=1),
    )
    quarters = exchange(to_everyone(placed, PER_GROUP), "tp", same_group)
    write_part = quarters[0] + quarters[1]
    read_part = quarters[2] + quarters[3]

    inner_window = jnp.concatenate([inner_history, inner_part[:, None, :]], axis=1)
    inner_conv = jax.nn.silu(
        jnp.sum(inner_window.astype(F32) * inner_taps.astype(F32)[None], axis=1)
    )
    history_own = slice_at(access_history, group * STATE, STATE, 3).astype(F32)
    taps_own = slice_at(access_taps, group * STATE, STATE, 2).astype(F32)

    def access_conv(which, part):
        taps = taps_own[which]
        past = jnp.sum(history_own[:, which] * taps[None, :3], axis=1)
        return jax.nn.silu(past + part.astype(F32) * taps[3][None])

    write_conv = access_conv(0, write_part)
    read_conv = access_conv(1, read_part)
    bias_own = slice_at(step_bias, tp, 1, 0)
    rate_own = slice_at(decay_log, tp, 1, 0)
    skip_own = slice_at(skip_scale, tp, 1, 0)
    step = jax.nn.softplus(step_raw + bias_own)
    decay = jnp.exp(-step * jnp.exp(rate_own))
    new_recurrent = (
        decay[:, None, None] * recurrent[:, 0]
        + (step[:, None] * inner_conv)[..., None] * write_conv[:, None, :]
    )
    readout = jnp.sum(new_recurrent * read_conv[:, None, :], axis=-1) + skip_own * inner_conv
    gated = readout * jax.nn.silu(gate_part.astype(F32))
    head_out = rms_scale(gated, head_gain).astype(BF)

    partial_mix = dot32(head_out, mixer_out)
    mix_pieces = partial_mix.astype(BF).reshape(seqs, n_tp, cols).transpose(1, 0, 2)
    parts_sent = jnp.where(tp % 2 == 0, write_part, read_part)
    arrived = exchange(
        jnp.concatenate([mix_pieces, to_everyone(parts_sent, n_tp)], axis=1), "tp"
    )
    mixed = jnp.sum(arrived[:, :seqs].astype(F32), axis=0).astype(BF)
    parts_all = arrived[:, seqs:].reshape(GROUPS, PER_GROUP, seqs, STATE)[:, :2]
    parts_all = parts_all.transpose(2, 1, 0, 3).reshape(seqs, 2, 1, GROUPS * STATE)
    new_access = jnp.concatenate([access_history[:, :, 1:], parts_all], axis=2)

    resid = slice_at(tokens, tp * cols, cols, 1).astype(F32) + mixed.astype(F32)
    gain_own = slice_at(moe_gain, tp * cols, cols, 0)
    scaled = (resid * gain_own).astype(BF)
    scaled_own = exchange(to_everyone(scaled, chips), "ep", same_core)
    scaled_own = scaled_own.reshape(chips * seqs, cols)
    scaled_other = lax.ppermute(scaled_own, "ep", swap)
    scaled_all = jnp.concatenate([scaled_own, scaled_other], axis=0)

    own_routes = own_pack[:, rows_k + 1, : 4 * seqs].astype(F32)
    other_routes = other_pack[:, rows_k + 1, : 4 * seqs].astype(F32)
    routes = jnp.concatenate([own_routes, other_routes], axis=0)
    mine = ep.astype(F32)
    is_first = routes[:, :seqs] == mine
    is_second = routes[:, seqs : 2 * seqs] == mine
    first_all = routes[:, 2 * seqs : 3 * seqs] + routes[:, 3 * seqs :]
    weight = jnp.where(is_first, first_all, 1.0 - first_all)
    named = is_first | is_second
    earlier = (jnp.arange(seqs)[:, None] < jnp.arange(seqs)[None]).astype(BF)
    rank = dot32(named.astype(BF), earlier)
    key = jnp.where(named, rank, -1.0)
    total = n_ep * seqs
    place = jnp.arange(total)[None]
    tiled = (place % seqs == jnp.arange(seqs)[:, None]).astype(F32)
    own_block = place // seqs == jnp.arange(n_ep)[:, None]
    spread = jnp.dot(
        jnp.concatenate([key, weight], axis=0), tiled, precision=lax.Precision.HIGHEST
    )
    key_row = jnp.sum(jnp.where(own_block, spread[:n_ep], 0.0), axis=0, keepdims=True)
    weight_row = jnp.sum(jnp.where(own_block, spread[n_ep:], 0.0), axis=0, keepdims=True)
    slots = TOP * n_ep
    slot = jnp.arange(slots)[:, None]
    chosen = (slot // TOP == place // seqs) & (key_row == (slot % TOP).astype(F32))
    slot_weight = jnp.sum(jnp.where(chosen, weight_row, 0.0), axis=1, keepdims=True)
    chosen = chosen.astype(BF)

    units = dense_gate.shape[1]
    half = -(-(units + 2) // 128) * 128
    blend_col = slice_at(blend_vector, tp * cols, cols, 0)[:, None]
    both_dense = jnp.concatenate(
        [
            dense_gate,
            blend_col,
            jnp.zeros((cols, half - units - 1), BF),
            dense_up,
            jnp.zeros((cols, half - units), BF),
        ],
        axis=1,
    )
    plain = scaled_all.astype(F32) / gain_own
    square_sum = jnp.sum(plain * plain, axis=1, keepdims=True)
    dense_partial = dot32(scaled_all, both_dense)
    dense_partial = jnp.where(
        jnp.arange(2 * half)[None] == units + 1, square_sum, dense_partial
    ).astype(BF)
    expert_rows = dot32(chosen, scaled_all).astype(BF)
    quarter = slots * cols // (2 * half)
    expert_block = (
        expert_rows.reshape(slots // quarter, quarter, cols)
        .transpose(1, 0, 2)
        .reshape(quarter, 2 * half)
    )
    share = total // n_tp
    arrived = exchange(
        jnp.concatenate(
            [dense_partial.reshape(n_tp, share, 2 * half), to_everyone(expert_block, n_tp)],
            axis=1,
        ),
        "tp",
    )
    dense_inner = jnp.sum(arrived[:, :share].astype(F32), axis=0)
    rows = (
        arrived[:, share:]
        .reshape(n_tp, quarter, slots // quarter, cols)
        .transpose(2, 1, 0, 3)
        .reshape(slots, width)
    )
    plain_rows = rows.astype(F32) / moe_gain
    row_scale = lax.rsqrt(jnp.mean(plain_rows * plain_rows, axis=1, keepdims=True) + EPS)
    gate_vals = dot32(rows, expert_gate[0]) * row_scale
    up_vals = dot32(rows, expert_up[0]) * row_scale
    act = (jax.nn.silu(gate_vals) * up_vals).astype(BF)
    partial_out = dot32(act, expert_down[0]).astype(BF)
    out_pieces = partial_out.reshape(slots, n_tp, cols).transpose(1, 0, 2)
    scale = lax.rsqrt(dense_inner[:, units + 1 : units + 2] / width + EPS)
    blend = jax.nn.sigmoid(dense_inner[:, units : units + 1] * scale)
    dense_act = (
        blend * jax.nn.silu(dense_inner[:, :half] * scale) * (dense_inner[:, half:] * scale)
    ).astype(BF)
    act_block = jnp.concatenate([dense_act[:, :128], dense_act[:, 128:]], axis=0)
    arrived = exchange(
        jnp.concatenate([out_pieces, to_everyone(act_block, n_tp)], axis=1), "tp"
    )
    expert_out = jnp.sum(arrived[:, :slots].astype(F32), axis=0) * slot_weight
    expert_out = expert_out.astype(BF)
    down = jnp.pad(dense_down, ((0, half - units), (0, 0)))

    def outputs_of(core_rank):
        acts = arrived[core_rank * n_tp // CORES : (core_rank + 1) * n_tp // CORES, slots:]
        tokens_of = total // CORES
        slots_of = slice(core_rank * slots // CORES, (core_rank + 1) * slots // CORES)
        picks = chosen[slots_of, core_rank * tokens_of : (core_rank + 1) * tokens_of]
        return (
            dot32(acts[:, :share].reshape(tokens_of, 128), down[:128])
            + dot32(acts[:, share:].reshape(tokens_of, 128), down[128:])
            + lax.dot_general(
                picks, expert_out[slots_of], (((0,), (0,)), ((), ())), preferred_element_type=F32
            )
        )

    swapped = lax.ppermute(outputs_of(1), "ep", swap)
    summed = outputs_of(0) + swapped
    final = exchange(summed.astype(BF).reshape(chips, seqs, cols), "ep", same_core)
    output = resid + jnp.sum(final.astype(F32), axis=0)
    return (output, new_recurrent[:, None], inner_window[:, 1:], new_access)


def solution(mesh):
    in_specs = (
        P("ep", None),
        P(),
        P("ep", "tp"),
        P("ep", "tp"),
        P("ep", None),
        P("ep", None),
        P("ep", None),
        P(),
        P(),
        P(),
        P(None, "tp"),
        P(),
        P("ep", None, "tp"),
        P("ep", None, None, None),
        P("ep", "tp", None, None),
        P("tp"),
        P("tp", None),
        P(),
        P("ep", None),
        P("ep", None),
        P("ep", None, "tp"),
        P("ep", None, "tp"),
        P("ep", "tp", None),
        P(),
        P("tp", "ep"),
        P("tp", "ep"),
        P("ep", "tp"),
    )
    out_specs = (
        P("ep", "tp"),
        P("ep", "tp", None, None),
        P("ep", None, "tp"),
        P("ep", None, None, None),
    )
    return jax.shard_map(local, mesh=mesh, in_specs=in_specs, out_specs=out_specs, check_vma=False)
```

```python
import jax
import jax.numpy as jnp
from jax import lax
from jax.sharding import PartitionSpec as P

HEADS = 16
HEAD_DIM = 64
GROUPS = 4
STATE = 128
TOP = 2
PER_GROUP = HEADS // GROUPS
EPS = 1e-06
BF = jnp.bfloat16
F32 = jnp.float32
CORES = 2


def exchange(pieces, axis, groups=None):
    return lax.all_to_all(
        pieces, axis, split_axis=0, concat_axis=0, tiled=True, axis_index_groups=groups
    )


def to_everyone(shard, peers):
    return jnp.broadcast_to(shard[None], (peers, *shard.shape))


def rms_scale(values, gain):
    mean_square = jnp.mean(values * values, axis=-1, keepdims=True)
    return values * lax.rsqrt(mean_square + EPS) * gain


def dot32(left, right):
    return jnp.dot(left, right, preferred_element_type=F32)


def slice_at(array, start, size, dim):
    return lax.dynamic_slice_in_dim(array, start, size, dim)


def local(
    tokens,
    mix_gain,
    gate_weight,
    inner_weight,
    write_weight,
    read_weight,
    step_weight,
    step_bias,
    decay_log,
    skip_scale,
    inner_taps,
    access_taps,
    inner_history,
    access_history,
    recurrent,
    head_gain,
    mixer_out,
    moe_gain,
    expert_ids,
    route_scores,
    expert_gate,
    expert_up,
    expert_down,
    blend_vector,
    dense_gate,
    dense_up,
    dense_down,
):
    seqs, width = tokens.shape
    n_ep = lax.axis_size("ep")
    n_tp = lax.axis_size("tp")
    chips = n_ep // CORES
    ep = lax.axis_index("ep")
    tp = lax.axis_index("tp")
    core = ep % CORES
    group = tp // PER_GROUP
    member = tp % PER_GROUP
    rows_k = gate_weight.shape[0]
    cols = width // n_tp
    same_core = [[CORES * z + c for z in range(chips)] for c in range(CORES)]

    def from_other_core(shard):
        return lax.ppermute(shard, "ep", [(i, i ^ 1) for i in range(n_ep)])

    same_group = [[PER_GROUP * g + m for m in range(PER_GROUP)] for g in range(GROUPS)]
    part = 2 * STATE // PER_GROUP

    write_own = slice_at(write_weight, group * STATE, STATE, 1)
    read_own = slice_at(read_weight, group * STATE, STATE, 1)
    either = jnp.where(member < PER_GROUP // 2, write_own, read_own)
    either = jnp.where(member % 2 == 0, either[:, :part], either[:, part:])
    main = jnp.concatenate([gate_weight, inner_weight, either], axis=1)
    pack_cols = main.shape[1]
    head_pick = (jnp.arange(HEADS) == tp).astype(BF)[None]
    step_row = lax.dot_general(
        head_pick, step_weight, (((1,), (1,)), ((), ())), preferred_element_type=F32
    ).astype(BF)
    first = jax.nn.sigmoid(route_scores[:, 0] - route_scores[:, 1])
    first_high = lax.reduce_precision(first, 8, 7)
    first_low = first - first_high
    lane = jnp.arange(4 * seqs)[None]
    spread = jnp.where(
        lane < seqs,
        expert_ids[:, 0:1].astype(F32),
        jnp.where(
            lane < 2 * seqs,
            expert_ids[:, 1:2].astype(F32),
            jnp.where(lane < 3 * seqs, first_high[:, None], first_low[:, None]),
        ),
    )
    route_row = jnp.sum(
        jnp.where(lane % seqs == jnp.arange(seqs)[:, None], spread, 0.0), axis=0, keepdims=True
    ).astype(BF)
    extra = jnp.concatenate([step_row, route_row, jnp.zeros((6, rows_k), BF)], axis=0)
    extra = jnp.pad(extra, ((0, 0), (0, pack_cols - rows_k)))
    pack = jnp.concatenate([main, extra], axis=0)
    own_pack = exchange(to_everyone(pack, chips), "ep", same_core)
    other_pack = from_other_core(own_pack)

    normed = rms_scale(tokens.astype(F32), mix_gain).astype(BF)
    by_core = normed.reshape(seqs, chips, CORES, rows_k)
    own_k = jnp.where(core == 0, by_core[:, :, 0], by_core[:, :, 1])
    other_k = jnp.where(core == 0, by_core[:, :, 1], by_core[:, :, 0])

    def projected_by(keys, packed):
        padded = jnp.pad(keys, ((0, 0), (0, 0), (0, packed.shape[1] - rows_k)))
        main_part = dot32(padded.reshape(seqs, -1), packed.reshape(-1, pack_cols))
        weights = packed[:, rows_k, :rows_k].astype(F32)
        step_part = jnp.sum(keys.astype(F32) * weights[None], axis=(1, 2))
        return main_part, step_part

    main_a, step_a = projected_by(own_k, own_pack)
    main_b, step_b = projected_by(other_k, other_pack)
    projected = main_a + main_b
    step_raw = step_a + step_b
    gate_part = projected[:, :HEAD_DIM].astype(BF)
    inner_part = projected[:, HEAD_DIM : 2 * HEAD_DIM].astype(BF)
    share_part = projected[:, 2 * HEAD_DIM :].astype(BF)
    none = jnp.zeros_like(share_part)
    placed = jnp.where(
        member % 2 == 0,
        jnp.concatenate([share_part, none], axis=1),
        jnp.concatenate([none, share_part], axis=1),
    )
    quarters = exchange(to_everyone(placed, PER_GROUP), "tp", same_group)
    write_part = quarters[0] + quarters[1]
    read_part = quarters[2] + quarters[3]

    inner_window = jnp.concatenate([inner_history, inner_part[:, None, :]], axis=1)
    inner_conv = jax.nn.silu(
        jnp.sum(inner_window.astype(F32) * inner_taps.astype(F32)[None], axis=1)
    )
    history_own = slice_at(access_history, group * STATE, STATE, 3).astype(F32)
    taps_own = slice_at(access_taps, group * STATE, STATE, 2).astype(F32)

    def access_conv(which, part):
        taps = taps_own[which]
        past = jnp.sum(history_own[:, which] * taps[None, :3], axis=1)
        return jax.nn.silu(past + part.astype(F32) * taps[3][None])

    write_conv = access_conv(0, write_part)
    read_conv = access_conv(1, read_part)
    bias_own = slice_at(step_bias, tp, 1, 0)
    rate_own = slice_at(decay_log, tp, 1, 0)
    skip_own = slice_at(skip_scale, tp, 1, 0)
    step = jax.nn.softplus(step_raw + bias_own)
    decay = jnp.exp(-step * jnp.exp(rate_own))
    new_recurrent = (
        decay[:, None, None] * recurrent[:, 0]
        + (step[:, None] * inner_conv)[..., None] * write_conv[:, None, :]
    )
    readout = jnp.sum(new_recurrent * read_conv[:, None, :], axis=-1) + skip_own * inner_conv
    gated = readout * jax.nn.silu(gate_part.astype(F32))
    head_out = rms_scale(gated, head_gain).astype(BF)

    total = chips * seqs
    at = jnp.arange(total)[:, None]
    by_source = (at // seqs == jnp.arange(chips)[None]).astype(BF)
    route_rows = dot32(by_source, own_pack[:, gate_weight.shape[0] + 1, : 4 * seqs])
    route_lane = jnp.arange(4 * seqs)[None]
    class_routes = jnp.concatenate(
        [
            jnp.sum(
                jnp.where(route_lane == which * seqs + at % seqs, route_rows, 0.0),
                axis=1,
                keepdims=True,
            )
            for which in range(4)
        ],
        axis=1,
    )

    units = CORES * dense_gate.shape[1]
    gate_pair = [expert_gate[0], from_other_core(expert_gate[0])]
    up_pair = [expert_up[0], from_other_core(expert_up[0])]
    down_pair = [expert_down[0], from_other_core(expert_down[0])]
    own_dense = jnp.concatenate([dense_gate, dense_up], axis=1)
    other_dense = from_other_core(own_dense)
    chip_down = jnp.concatenate([dense_down, from_other_core(dense_down)], axis=0)

    partial_mix = dot32(head_out, mixer_out)
    mix_pieces = partial_mix.astype(BF).reshape(seqs, n_tp, cols).transpose(1, 0, 2)
    parts_sent = jnp.where(tp % 2 == 0, write_part, read_part)
    arrived = exchange(
        jnp.concatenate([mix_pieces, to_everyone(parts_sent, n_tp)], axis=1), "tp"
    )
    mixed = jnp.sum(arrived[:, :seqs].astype(F32), axis=0).astype(BF)
    parts_all = arrived[:, seqs:].reshape(GROUPS, PER_GROUP, seqs, STATE)[:, :2]
    parts_all = parts_all.transpose(2, 1, 0, 3).reshape(seqs, 2, 1, GROUPS * STATE)
    new_access = jnp.concatenate([access_history[:, :, 1:], parts_all], axis=2)

    resid = slice_at(tokens, tp * cols, cols, 1).astype(F32) + mixed.astype(F32)
    gain_own = slice_at(moe_gain, tp * cols, cols, 0)
    scaled = (resid * gain_own).astype(BF)
    class_scaled = exchange(to_everyone(scaled, chips), "ep", same_core).reshape(total, cols)

    first_all = class_routes[:, 2:3] + class_routes[:, 3:4]
    place = jnp.arange(total)
    block = place // seqs
    earlier = ((block[:, None] == block[None]) & (place[None] < place[:, None])).astype(BF)
    mine = jnp.stack([ep, ep + 1 - 2 * core]).astype(F32)[None]
    is_first = class_routes[:, 0:1] == mine
    named = is_first | (class_routes[:, 1:2] == mine)
    weight = jnp.where(is_first, first_all, 1.0 - first_all)
    weight_high = lax.reduce_precision(weight, 8, 7)
    weight_low = (weight - weight_high).astype(BF)
    rank = jnp.where(named, dot32(earlier, named.astype(BF)), -1.0)
    per_expert = TOP * chips
    slots = CORES * per_expert
    slot = jnp.arange(slots)[None]
    key = jnp.where(slot < per_expert, rank[:, 0:1], rank[:, 1:2])
    chosen = (slot % per_expert // TOP == block[:, None]) & (key == (slot % TOP).astype(F32))
    chosen = chosen.astype(BF)
    by_slot = lax.dot_general(
        chosen,
        jnp.concatenate([weight_high.astype(BF), weight_low], axis=1),
        (((0,), (0,)), ((), ())),
        preferred_element_type=F32,
    )
    slot_weight = jnp.where(
        jnp.arange(slots)[:, None] < per_expert,
        by_slot[:, 0:1] + by_slot[:, 2:3],
        by_slot[:, 1:2] + by_slot[:, 3:4],
    )

    half = -(-(units + 2) // 128) * 128
    own_units = units // CORES
    blend_col = slice_at(blend_vector, tp * cols, cols, 0)[:, None]
    both_dense = jnp.concatenate(
        [
            own_dense[:, :own_units],
            other_dense[:, :own_units],
            blend_col,
            jnp.zeros((cols, half - units - 1), BF),
            own_dense[:, own_units:],
            other_dense[:, own_units:],
            jnp.zeros((cols, half - units), BF),
        ],
        axis=1,
    )
    plain = class_scaled.astype(F32) / gain_own
    square_sum = jnp.sum(plain * plain, axis=1, keepdims=True)
    dense_partial = dot32(class_scaled, both_dense)
    dense_partial = jnp.where(
        jnp.arange(2 * half)[None] == units + 1, square_sum, dense_partial
    ).astype(BF)
    expert_rows = lax.dot_general(
        chosen, class_scaled, (((0,), (0,)), ((), ())), preferred_element_type=F32
    ).astype(BF)
    wide = 2 * half // cols
    deep = slots // wide
    expert_block = (
        expert_rows.reshape(wide, deep, cols).transpose(1, 0, 2).reshape(deep, 2 * half)
    )
    share = total // n_tp
    arrived = exchange(
        jnp.concatenate(
            [dense_partial.reshape(n_tp, share, 2 * half), to_everyone(expert_block, n_tp)],
            axis=1,
        ),
        "tp",
    )
    dense_inner = jnp.sum(arrived[:, :share].astype(F32), axis=0)
    rows = (
        arrived[:, share:]
        .reshape(n_tp, deep, wide, cols)
        .transpose(2, 1, 0, 3)
        .reshape(slots, width)
    )
    plain_rows = rows.astype(F32) / moe_gain
    row_scale = lax.rsqrt(jnp.mean(plain_rows * plain_rows, axis=1, keepdims=True) + EPS)

    def expert_share(which):
        here = slice(which * per_expert, (which + 1) * per_expert)
        gate_vals = dot32(rows[here], gate_pair[which]) * row_scale[here]
        up_vals = dot32(rows[here], up_pair[which]) * row_scale[here]
        act = (jax.nn.silu(gate_vals) * up_vals).astype(BF)
        return dot32(act, down_pair[which]).astype(BF)

    partial_out = jnp.concatenate([expert_share(0), expert_share(1)], axis=0)
    out_pieces = partial_out.reshape(slots, n_tp, cols).transpose(1, 0, 2)
    scale = lax.rsqrt(dense_inner[:, units + 1 : units + 2] / width + EPS)
    blend = jax.nn.sigmoid(dense_inner[:, units : units + 1] * scale)
    dense_act = (
        blend * jax.nn.silu(dense_inner[:, :half] * scale) * (dense_inner[:, half:] * scale)
    ).astype(BF)
    tiles = half // 128
    act_block = dense_act.reshape(share, tiles, 128).transpose(1, 0, 2).reshape(tiles * share, 128)
    arrived = exchange(
        jnp.concatenate([out_pieces, to_everyone(act_block, n_tp)], axis=1), "tp"
    )
    expert_out = jnp.sum(arrived[:, :slots].astype(F32), axis=0) * slot_weight
    act_all = (
        arrived[:, slots:]
        .reshape(n_tp, tiles, share, 128)
        .transpose(0, 2, 1, 3)
        .reshape(total, half)
    )
    down = jnp.pad(chip_down, ((0, half - units), (0, 0)))
    summed = dot32(act_all, down) + dot32(chosen, expert_out.astype(BF))
    final = exchange(summed.astype(BF).reshape(chips, seqs, cols), "ep", same_core)
    output = resid + jnp.sum(final.astype(F32), axis=0)
    return (output, new_recurrent[:, None], inner_window[:, 1:], new_access)


def solution(mesh):
    in_specs = (
        P("ep", None),
        P(),
        P("ep", "tp"),
        P("ep", "tp"),
        P("ep", None),
        P("ep", None),
        P("ep", None),
        P(),
        P(),
        P(),
        P(None, "tp"),
        P(),
        P("ep", None, "tp"),
        P("ep", None, None, None),
        P("ep", "tp", None, None),
        P("tp"),
        P("tp", None),
        P(),
        P("ep", None),
        P("ep", None),
        P("ep", None, "tp"),
        P("ep", None, "tp"),
        P("ep", "tp", None),
        P(),
        P("tp", "ep"),
        P("tp", "ep"),
        P("ep", "tp"),
    )
    out_specs = (
        P("ep", "tp"),
        P("ep", "tp", None, None),
        P("ep", None, "tp"),
        P("ep", None, None, None),
    )
    return jax.shard_map(local, mesh=mesh, in_specs=in_specs, out_specs=out_specs, check_vma=False)
```

```python
import jax
import jax.numpy as jnp
from jax import lax
from jax.sharding import PartitionSpec as P

HEADS = 16
HEAD_DIM = 64
GROUPS = 4
STATE = 128
TOP = 2
PER_GROUP = HEADS // GROUPS
EPS = 1e-06
BF = jnp.bfloat16
F32 = jnp.float32
CORES = 2
CLASSES = 8


def exchange(pieces, axis, groups=None):
    return lax.all_to_all(
        pieces, axis, split_axis=0, concat_axis=0, tiled=True, axis_index_groups=groups
    )


def to_everyone(shard, peers):
    return jnp.broadcast_to(shard[None], (peers, *shard.shape))


def rms_scale(values, gain):
    mean_square = jnp.mean(values * values, axis=-1, keepdims=True)
    return values * lax.rsqrt(mean_square + EPS) * gain


def dot32(left, right):
    return jnp.dot(left, right, preferred_element_type=F32)


def slice_at(array, start, size, dim):
    return lax.dynamic_slice_in_dim(array, start, size, dim)


def local(
    tokens,
    mix_gain,
    gate_weight,
    inner_weight,
    write_weight,
    read_weight,
    step_weight,
    step_bias,
    decay_log,
    skip_scale,
    inner_taps,
    access_taps,
    inner_history,
    access_history,
    recurrent,
    head_gain,
    mixer_out,
    moe_gain,
    expert_ids,
    route_scores,
    expert_gate,
    expert_up,
    expert_down,
    blend_vector,
    dense_gate,
    dense_up,
    dense_down,
):
    seqs, width = tokens.shape
    n_ep = lax.axis_size("ep")
    n_tp = lax.axis_size("tp")
    chips = n_ep // CORES
    ep = lax.axis_index("ep")
    tp = lax.axis_index("tp")
    core = ep % CORES
    group = tp // PER_GROUP
    rows_k = gate_weight.shape[0]
    cols = width // n_tp
    same_core = [[CORES * z + c for z in range(chips)] for c in range(CORES)]

    def from_other_core(shard):
        return lax.ppermute(shard, "ep", [(i, i ^ 1) for i in range(n_ep)])

    per_class = n_ep // CLASSES
    same_class = [[CLASSES * j + r for j in range(per_class)] for r in range(CLASSES)]
    near = [[CLASSES * j + r for r in range(CLASSES)] for j in range(per_class)]

    write_own = slice_at(write_weight, group * STATE, STATE, 1)
    read_own = slice_at(read_weight, group * STATE, STATE, 1)
    main = jnp.concatenate([gate_weight, inner_weight, write_own, read_own], axis=1)
    pack_cols = main.shape[1]
    head_pick = (jnp.arange(HEADS) == tp).astype(BF)[None]
    step_row = lax.dot_general(
        head_pick, step_weight, (((1,), (1,)), ((), ())), preferred_element_type=F32
    ).astype(BF)
    first = jax.nn.sigmoid(route_scores[:, 0] - route_scores[:, 1])
    first_high = lax.reduce_precision(first, 8, 7)
    first_low = first - first_high
    lane = jnp.arange(4 * seqs)[None]
    spread = jnp.where(
        lane < seqs,
        expert_ids[:, 0:1].astype(F32),
        jnp.where(
            lane < 2 * seqs,
            expert_ids[:, 1:2].astype(F32),
            jnp.where(lane < 3 * seqs, first_high[:, None], first_low[:, None]),
        ),
    )
    route_row = jnp.sum(
        jnp.where(lane % seqs == jnp.arange(seqs)[:, None], spread, 0.0), axis=0, keepdims=True
    ).astype(BF)
    extra = jnp.concatenate([step_row, route_row, jnp.zeros((6, rows_k), BF)], axis=0)
    extra = jnp.pad(extra, ((0, 0), (0, pack_cols - rows_k)))
    pack = jnp.concatenate([main, extra], axis=0)
    class_pack = exchange(to_everyone(pack, per_class), "ep", same_class)

    normed = rms_scale(tokens.astype(F32), mix_gain).astype(BF)
    keys = normed.reshape(seqs, per_class, CLASSES, rows_k).transpose(2, 0, 1, 3)
    keys = exchange(keys.reshape(CLASSES, seqs, per_class * rows_k), "ep", near)
    keys = keys.reshape(CLASSES * seqs, per_class, rows_k)
    padded = jnp.pad(keys, ((0, 0), (0, 0), (0, pack.shape[0] - rows_k)))
    main_share = dot32(padded.reshape(CLASSES * seqs, -1), class_pack.reshape(-1, pack_cols))
    step_rows = class_pack[:, rows_k, :rows_k].astype(F32)
    step_share = jnp.sum(keys.astype(F32) * step_rows[None], axis=(1, 2)).reshape(CLASSES, seqs, 1)
    route_rows = class_pack[:, rows_k + 1, : 4 * seqs].astype(F32)
    route_rows = jnp.pad(route_rows, ((0, seqs - per_class), (0, 0)))
    shares = exchange(
        jnp.concatenate(
            [
                main_share.reshape(CLASSES, seqs, pack_cols),
                step_share,
                jnp.zeros((CLASSES, seqs, 63), F32),
                to_everyone(route_rows, CLASSES),
            ],
            axis=2,
        ),
        "ep",
        near,
    )
    projected = jnp.sum(shares[:, :, : pack_cols + 1], axis=0)
    step_raw = projected[:, pack_cols]
    own_routes = lax.dynamic_index_in_dim(
        shares[:, :per_class, pack_cols + 64 :].reshape(
            CLASSES // CORES, CORES, per_class, 4 * seqs
        ),
        core,
        1,
        False,
    )
    own_routes = own_routes.transpose(1, 0, 2).reshape(chips, 4 * seqs)
    gate_part = projected[:, :HEAD_DIM].astype(BF)
    inner_part = projected[:, HEAD_DIM : 2 * HEAD_DIM].astype(BF)
    write_part = projected[:, 2 * HEAD_DIM : 2 * HEAD_DIM + STATE].astype(BF)
    read_part = projected[:, 2 * HEAD_DIM + STATE : pack_cols].astype(BF)

    inner_window = jnp.concatenate([inner_history, inner_part[:, None, :]], axis=1)
    inner_conv = jax.nn.silu(
        jnp.sum(inner_window.astype(F32) * inner_taps.astype(F32)[None], axis=1)
    )
    history_own = slice_at(access_history, group * STATE, STATE, 3).astype(F32)
    taps_own = slice_at(access_taps, group * STATE, STATE, 2).astype(F32)

    def access_conv(which, part):
        taps = taps_own[which]
        past = jnp.sum(history_own[:, which] * taps[None, :3], axis=1)
        return jax.nn.silu(past + part.astype(F32) * taps[3][None])

    write_conv = access_conv(0, write_part)
    read_conv = access_conv(1, read_part)
    bias_own = slice_at(step_bias, tp, 1, 0)
    rate_own = slice_at(decay_log, tp, 1, 0)
    skip_own = slice_at(skip_scale, tp, 1, 0)
    step = jax.nn.softplus(step_raw + bias_own)
    decay = jnp.exp(-step * jnp.exp(rate_own))
    new_recurrent = (
        decay[:, None, None] * recurrent[:, 0]
        + (step[:, None] * inner_conv)[..., None] * write_conv[:, None, :]
    )
    readout = jnp.sum(new_recurrent * read_conv[:, None, :], axis=-1) + skip_own * inner_conv
    gated = readout * jax.nn.silu(gate_part.astype(F32))
    head_out = rms_scale(gated, head_gain).astype(BF)

    total = chips * seqs
    at = jnp.arange(total)[:, None]
    by_source = (at // seqs == jnp.arange(chips)[None]).astype(BF)
    route_rows = dot32(by_source, own_routes.astype(BF))
    route_lane = jnp.arange(4 * seqs)[None]
    class_routes = jnp.concatenate(
        [
            jnp.sum(
                jnp.where(route_lane == which * seqs + at % seqs, route_rows, 0.0),
                axis=1,
                keepdims=True,
            )
            for which in range(4)
        ],
        axis=1,
    )

    units = CORES * dense_gate.shape[1]
    gate_pair = [expert_gate[0], from_other_core(expert_gate[0])]
    up_pair = [expert_up[0], from_other_core(expert_up[0])]
    down_pair = [expert_down[0], from_other_core(expert_down[0])]
    own_dense = jnp.concatenate([dense_gate, dense_up], axis=1)
    other_dense = from_other_core(own_dense)
    chip_down = jnp.concatenate([dense_down, from_other_core(dense_down)], axis=0)

    partial_mix = dot32(head_out, mixer_out)
    mix_pieces = partial_mix.astype(BF).reshape(seqs, n_tp, cols).transpose(1, 0, 2)
    parts_sent = jnp.where(tp % 2 == 0, write_part, read_part)
    arrived = exchange(
        jnp.concatenate([mix_pieces, to_everyone(parts_sent, n_tp)], axis=1), "tp"
    )
    mixed = jnp.sum(arrived[:, :seqs].astype(F32), axis=0).astype(BF)
    parts_all = arrived[:, seqs:].reshape(GROUPS, PER_GROUP, seqs, STATE)[:, :2]
    parts_all = parts_all.transpose(2, 1, 0, 3).reshape(seqs, 2, 1, GROUPS * STATE)
    new_access = jnp.concatenate([access_history[:, :, 1:], parts_all], axis=2)

    resid = slice_at(tokens, tp * cols, cols, 1).astype(F32) + mixed.astype(F32)
    gain_own = slice_at(moe_gain, tp * cols, cols, 0)
    scaled = (resid * gain_own).astype(BF)
    class_scaled = exchange(to_everyone(scaled, chips), "ep", same_core).reshape(total, cols)

    first_all = class_routes[:, 2:3] + class_routes[:, 3:4]
    place = jnp.arange(total)
    block = place // seqs
    earlier = ((block[:, None] == block[None]) & (place[None] < place[:, None])).astype(BF)
    mine = jnp.stack([ep, ep + 1 - 2 * core]).astype(F32)[None]
    is_first = class_routes[:, 0:1] == mine
    named = is_first | (class_routes[:, 1:2] == mine)
    weight = jnp.where(is_first, first_all, 1.0 - first_all)
    weight_high = lax.reduce_precision(weight, 8, 7)
    weight_low = (weight - weight_high).astype(BF)
    rank = jnp.where(named, dot32(earlier, named.astype(BF)), -1.0)
    per_expert = TOP * chips
    slots = CORES * per_expert
    slot = jnp.arange(slots)[None]
    key = jnp.where(slot < per_expert, rank[:, 0:1], rank[:, 1:2])
    chosen = (slot % per_expert // TOP == block[:, None]) & (key == (slot % TOP).astype(F32))
    chosen = chosen.astype(BF)
    by_slot = lax.dot_general(
        chosen,
        jnp.concatenate([weight_high.astype(BF), weight_low], axis=1),
        (((0,), (0,)), ((), ())),
        preferred_element_type=F32,
    )
    slot_weight = jnp.where(
        jnp.arange(slots)[:, None] < per_expert,
        by_slot[:, 0:1] + by_slot[:, 2:3],
        by_slot[:, 1:2] + by_slot[:, 3:4],
    )

    half = -(-(units + 2) // 128) * 128
    own_units = units // CORES
    blend_col = slice_at(blend_vector, tp * cols, cols, 0)[:, None]
    both_dense = jnp.concatenate(
        [
            own_dense[:, :own_units],
            other_dense[:, :own_units],
            blend_col,
            jnp.zeros((cols, half - units - 1), BF),
            own_dense[:, own_units:],
            other_dense[:, own_units:],
            jnp.zeros((cols, half - units), BF),
        ],
        axis=1,
    )
    plain = class_scaled.astype(F32) / gain_own
    square_sum = jnp.sum(plain * plain, axis=1, keepdims=True)
    dense_partial = dot32(class_scaled, both_dense)
    dense_partial = jnp.where(
        jnp.arange(2 * half)[None] == units + 1, square_sum, dense_partial
    ).astype(BF)
    expert_rows = lax.dot_general(
        chosen, class_scaled, (((0,), (0,)), ((), ())), preferred_element_type=F32
    ).astype(BF)
    wide = 2 * half // cols
    deep = slots // wide
    expert_block = (
        expert_rows.reshape(wide, deep, cols).transpose(1, 0, 2).reshape(deep, 2 * half)
    )
    share = total // n_tp
    arrived = exchange(
        jnp.concatenate(
            [dense_partial.reshape(n_tp, share, 2 * half), to_everyone(expert_block, n_tp)],
            axis=1,
        ),
        "tp",
    )
    dense_inner = jnp.sum(arrived[:, :share].astype(F32), axis=0)
    rows = (
        arrived[:, share:]
        .reshape(n_tp, deep, wide, cols)
        .transpose(2, 1, 0, 3)
        .reshape(slots, width)
    )
    plain_rows = rows.astype(F32) / moe_gain
    row_scale = lax.rsqrt(jnp.mean(plain_rows * plain_rows, axis=1, keepdims=True) + EPS)

    def expert_share(which):
        here = slice(which * per_expert, (which + 1) * per_expert)
        gate_vals = dot32(rows[here], gate_pair[which]) * row_scale[here]
        up_vals = dot32(rows[here], up_pair[which]) * row_scale[here]
        act = (jax.nn.silu(gate_vals) * up_vals).astype(BF)
        return dot32(act, down_pair[which]).astype(BF)

    partial_out = jnp.concatenate([expert_share(0), expert_share(1)], axis=0)
    out_pieces = partial_out.reshape(slots, n_tp, cols).transpose(1, 0, 2)
    scale = lax.rsqrt(dense_inner[:, units + 1 : units + 2] / width + EPS)
    blend = jax.nn.sigmoid(dense_inner[:, units : units + 1] * scale)
    dense_act = (
        blend * jax.nn.silu(dense_inner[:, :half] * scale) * (dense_inner[:, half:] * scale)
    ).astype(BF)
    tiles = half // 128
    act_block = dense_act.reshape(share, tiles, 128).transpose(1, 0, 2).reshape(tiles * share, 128)
    arrived = exchange(
        jnp.concatenate([out_pieces, to_everyone(act_block, n_tp)], axis=1), "tp"
    )
    expert_out = jnp.sum(arrived[:, :slots].astype(F32), axis=0) * slot_weight
    act_all = (
        arrived[:, slots:]
        .reshape(n_tp, tiles, share, 128)
        .transpose(0, 2, 1, 3)
        .reshape(total, half)
    )
    down = jnp.pad(chip_down, ((0, half - units), (0, 0)))
    summed = dot32(act_all, down) + dot32(chosen, expert_out.astype(BF))
    final = exchange(summed.astype(BF).reshape(chips, seqs, cols), "ep", same_core)
    output = resid + jnp.sum(final.astype(F32), axis=0)
    return (output, new_recurrent[:, None], inner_window[:, 1:], new_access)


def solution(mesh):
    in_specs = (
        P("ep", None),
        P(),
        P("ep", "tp"),
        P("ep", "tp"),
        P("ep", None),
        P("ep", None),
        P("ep", None),
        P(),
        P(),
        P(),
        P(None, "tp"),
        P(),
        P("ep", None, "tp"),
        P("ep", None, None, None),
        P("ep", "tp", None, None),
        P("tp"),
        P("tp", None),
        P(),
        P("ep", None),
        P("ep", None),
        P("ep", None, "tp"),
        P("ep", None, "tp"),
        P("ep", "tp", None),
        P(),
        P("tp", "ep"),
        P("tp", "ep"),
        P("ep", "tp"),
    )
    out_specs = (
        P("ep", "tp"),
        P("ep", "tp", None, None),
        P("ep", None, "tp"),
        P("ep", None, None, None),
    )
    return jax.shard_map(local, mesh=mesh, in_specs=in_specs, out_specs=out_specs, check_vma=False)
```

```python
import jax
import jax.numpy as jnp
from jax import lax
from jax.sharding import PartitionSpec as P

HEADS = 16
HEAD_DIM = 64
GROUPS = 4
STATE = 128
TOP = 2
PER_GROUP = HEADS // GROUPS
EPS = 1e-06
BF = jnp.bfloat16
F32 = jnp.float32
CORES = 2
CLASSES = 8


def exchange(pieces, axis, groups=None):
    return lax.all_to_all(
        pieces, axis, split_axis=0, concat_axis=0, tiled=True, axis_index_groups=groups
    )


def to_everyone(shard, peers):
    return jnp.broadcast_to(shard[None], (peers, *shard.shape))


def rms_scale(values, gain):
    mean_square = jnp.mean(values * values, axis=-1, keepdims=True)
    return values * lax.rsqrt(mean_square + EPS) * gain


def dot32(left, right):
    return jnp.dot(left, right, preferred_element_type=F32)


def slice_at(array, start, size, dim):
    return lax.dynamic_slice_in_dim(array, start, size, dim)


def local(
    tokens,
    mix_gain,
    gate_weight,
    inner_weight,
    write_weight,
    read_weight,
    step_weight,
    step_bias,
    decay_log,
    skip_scale,
    inner_taps,
    access_taps,
    inner_history,
    access_history,
    recurrent,
    head_gain,
    mixer_out,
    moe_gain,
    expert_ids,
    route_scores,
    expert_gate,
    expert_up,
    expert_down,
    blend_vector,
    dense_gate,
    dense_up,
    dense_down,
):
    seqs, width = tokens.shape
    n_ep = lax.axis_size("ep")
    n_tp = lax.axis_size("tp")
    chips = n_ep // CORES
    ep = lax.axis_index("ep")
    tp = lax.axis_index("tp")
    core = ep % CORES
    group = tp // PER_GROUP
    rows_k = gate_weight.shape[0]
    cols = width // n_tp
    same_core = [[CORES * z + c for z in range(chips)] for c in range(CORES)]

    def from_other_core(shard):
        return lax.ppermute(shard, "ep", [(i, i ^ 1) for i in range(n_ep)])

    per_class = n_ep // CLASSES
    first_class = ep // CLASSES
    near = [[CLASSES * j + r for r in range(CLASSES)] for j in range(per_class)]

    write_own = slice_at(write_weight, group * STATE, STATE, 1)
    read_own = slice_at(read_weight, group * STATE, STATE, 1)
    main = jnp.concatenate([gate_weight, inner_weight, write_own, read_own], axis=1)
    pack_cols = main.shape[1]
    head_pick = (jnp.arange(HEADS) == tp).astype(BF)[None]
    step_row = lax.dot_general(
        head_pick, step_weight, (((1,), (1,)), ((), ())), preferred_element_type=F32
    ).astype(BF)
    first = jax.nn.sigmoid(route_scores[:, 0] - route_scores[:, 1])
    first_high = lax.reduce_precision(first, 8, 7)
    first_low = first - first_high
    lane = jnp.arange(4 * seqs)[None]
    spread = jnp.where(
        lane < seqs,
        expert_ids[:, 0:1].astype(F32),
        jnp.where(
            lane < 2 * seqs,
            expert_ids[:, 1:2].astype(F32),
            jnp.where(lane < 3 * seqs, first_high[:, None], first_low[:, None]),
        ),
    )
    route_row = jnp.sum(
        jnp.where(lane % seqs == jnp.arange(seqs)[:, None], spread, 0.0), axis=0, keepdims=True
    ).astype(BF)
    extra = jnp.concatenate([step_row, route_row, jnp.zeros((6, rows_k), BF)], axis=0)
    extra = jnp.pad(extra, ((0, 0), (0, pack_cols - rows_k)))
    pack = jnp.concatenate([main, extra], axis=0)
    class_pack = [pack]
    for ahead in range(1, per_class):
        hops = [(i, (i - CLASSES * ahead) % n_ep) for i in range(n_ep)]
        class_pack.append(lax.ppermute(pack, "ep", hops))
    class_pack = jnp.stack(class_pack)

    normed = rms_scale(tokens.astype(F32), mix_gain).astype(BF)
    rotated = slice_at(
        jnp.concatenate([normed, normed], axis=1), first_class * CLASSES * rows_k, width, 1
    )
    keys = rotated.reshape(seqs, per_class, CLASSES, rows_k).transpose(2, 0, 1, 3)
    keys = exchange(keys.reshape(CLASSES, seqs, per_class * rows_k), "ep", near)
    keys = keys.reshape(CLASSES * seqs, per_class, rows_k)
    padded = jnp.pad(keys, ((0, 0), (0, 0), (0, pack.shape[0] - rows_k)))
    main_share = dot32(padded.reshape(CLASSES * seqs, -1), class_pack.reshape(-1, pack_cols))
    step_rows = class_pack[:, rows_k, :rows_k].astype(F32)
    step_share = jnp.sum(keys.astype(F32) * step_rows[None], axis=(1, 2)).reshape(CLASSES, seqs, 1)
    route_rows = class_pack[:, rows_k + 1, : 4 * seqs].astype(F32)
    route_rows = jnp.pad(route_rows, ((0, seqs - per_class), (0, 0)))
    shares = exchange(
        jnp.concatenate(
            [
                main_share.reshape(CLASSES, seqs, pack_cols),
                step_share,
                jnp.zeros((CLASSES, seqs, 63), F32),
                to_everyone(route_rows, CLASSES),
            ],
            axis=2,
        ),
        "ep",
        near,
    )
    projected = jnp.sum(shares[:, :, : pack_cols + 1], axis=0)
    step_raw = projected[:, pack_cols]
    own_routes = lax.dynamic_index_in_dim(
        shares[:, :per_class, pack_cols + 64 :].reshape(
            CLASSES // CORES, CORES, per_class, 4 * seqs
        ),
        core,
        1,
        False,
    )
    own_routes = own_routes.transpose(1, 0, 2).reshape(chips, 4 * seqs)
    gate_part = projected[:, :HEAD_DIM].astype(BF)
    inner_part = projected[:, HEAD_DIM : 2 * HEAD_DIM].astype(BF)
    write_part = projected[:, 2 * HEAD_DIM : 2 * HEAD_DIM + STATE].astype(BF)
    read_part = projected[:, 2 * HEAD_DIM + STATE : pack_cols].astype(BF)

    inner_window = jnp.concatenate([inner_history, inner_part[:, None, :]], axis=1)
    inner_conv = jax.nn.silu(
        jnp.sum(inner_window.astype(F32) * inner_taps.astype(F32)[None], axis=1)
    )
    history_own = slice_at(access_history, group * STATE, STATE, 3).astype(F32)
    taps_own = slice_at(access_taps, group * STATE, STATE, 2).astype(F32)

    def access_conv(which, part):
        taps = taps_own[which]
        past = jnp.sum(history_own[:, which] * taps[None, :3], axis=1)
        return jax.nn.silu(past + part.astype(F32) * taps[3][None])

    write_conv = access_conv(0, write_part)
    read_conv = access_conv(1, read_part)
    bias_own = slice_at(step_bias, tp, 1, 0)
    rate_own = slice_at(decay_log, tp, 1, 0)
    skip_own = slice_at(skip_scale, tp, 1, 0)
    step = jax.nn.softplus(step_raw + bias_own)
    decay = jnp.exp(-step * jnp.exp(rate_own))
    new_recurrent = (
        decay[:, None, None] * recurrent[:, 0]
        + (step[:, None] * inner_conv)[..., None] * write_conv[:, None, :]
    )
    readout = jnp.sum(new_recurrent * read_conv[:, None, :], axis=-1) + skip_own * inner_conv
    gated = readout * jax.nn.silu(gate_part.astype(F32))
    head_out = rms_scale(gated, head_gain).astype(BF)

    total = chips * seqs
    at = jnp.arange(total)[:, None]
    source = (jnp.arange(chips)[None] + first_class * (CLASSES // CORES)) % chips
    by_source = (at // seqs == source).astype(BF)
    route_rows = dot32(by_source, own_routes.astype(BF))
    route_lane = jnp.arange(4 * seqs)[None]
    class_routes = jnp.concatenate(
        [
            jnp.sum(
                jnp.where(route_lane == which * seqs + at % seqs, route_rows, 0.0),
                axis=1,
                keepdims=True,
            )
            for which in range(4)
        ],
        axis=1,
    )

    units = CORES * dense_gate.shape[1]
    gate_pair = [expert_gate[0], from_other_core(expert_gate[0])]
    up_pair = [expert_up[0], from_other_core(expert_up[0])]
    down_pair = [expert_down[0], from_other_core(expert_down[0])]
    own_dense = jnp.concatenate([dense_gate, dense_up], axis=1)
    other_dense = from_other_core(own_dense)
    chip_down = jnp.concatenate([dense_down, from_other_core(dense_down)], axis=0)

    partial_mix = dot32(head_out, mixer_out)
    mix_pieces = partial_mix.astype(BF).reshape(seqs, n_tp, cols).transpose(1, 0, 2)
    parts_sent = jnp.where(tp % 2 == 0, write_part, read_part)
    arrived = exchange(
        jnp.concatenate([mix_pieces, to_everyone(parts_sent, n_tp)], axis=1), "tp"
    )
    mixed = jnp.sum(arrived[:, :seqs].astype(F32), axis=0).astype(BF)
    parts_all = arrived[:, seqs:].reshape(GROUPS, PER_GROUP, seqs, STATE)[:, :2]
    parts_all = parts_all.transpose(2, 1, 0, 3).reshape(seqs, 2, 1, GROUPS * STATE)
    new_access = jnp.concatenate([access_history[:, :, 1:], parts_all], axis=2)

    resid = slice_at(tokens, tp * cols, cols, 1).astype(F32) + mixed.astype(F32)
    gain_own = slice_at(moe_gain, tp * cols, cols, 0)
    scaled = (resid * gain_own).astype(BF)
    class_scaled = exchange(to_everyone(scaled, chips), "ep", same_core).reshape(total, cols)

    first_all = class_routes[:, 2:3] + class_routes[:, 3:4]
    place = jnp.arange(total)
    block = place // seqs
    earlier = ((block[:, None] == block[None]) & (place[None] < place[:, None])).astype(BF)
    mine = jnp.stack([ep, ep + 1 - 2 * core]).astype(F32)[None]
    is_first = class_routes[:, 0:1] == mine
    named = is_first | (class_routes[:, 1:2] == mine)
    weight = jnp.where(is_first, first_all, 1.0 - first_all)
    weight_high = lax.reduce_precision(weight, 8, 7)
    weight_low = (weight - weight_high).astype(BF)
    rank = jnp.where(named, dot32(earlier, named.astype(BF)), -1.0)
    per_expert = TOP * chips
    slots = CORES * per_expert
    slot = jnp.arange(slots)[None]
    key = jnp.where(slot < per_expert, rank[:, 0:1], rank[:, 1:2])
    chosen = (slot % per_expert // TOP == block[:, None]) & (key == (slot % TOP).astype(F32))
    chosen = chosen.astype(BF)
    by_slot = lax.dot_general(
        chosen,
        jnp.concatenate([weight_high.astype(BF), weight_low], axis=1),
        (((0,), (0,)), ((), ())),
        preferred_element_type=F32,
    )
    slot_weight = jnp.where(
        jnp.arange(slots)[:, None] < per_expert,
        by_slot[:, 0:1] + by_slot[:, 2:3],
        by_slot[:, 1:2] + by_slot[:, 3:4],
    )

    half = -(-(units + 2) // 128) * 128
    own_units = units // CORES
    blend_col = slice_at(blend_vector, tp * cols, cols, 0)[:, None]
    both_dense = jnp.concatenate(
        [
            own_dense[:, :own_units],
            other_dense[:, :own_units],
            blend_col,
            jnp.zeros((cols, half - units - 1), BF),
            own_dense[:, own_units:],
            other_dense[:, own_units:],
            jnp.zeros((cols, half - units), BF),
        ],
        axis=1,
    )
    plain = class_scaled.astype(F32) / gain_own
    square_sum = jnp.sum(plain * plain, axis=1, keepdims=True)
    dense_partial = dot32(class_scaled, both_dense)
    dense_partial = jnp.where(
        jnp.arange(2 * half)[None] == units + 1, square_sum, dense_partial
    ).astype(BF)
    expert_rows = lax.dot_general(
        chosen, class_scaled, (((0,), (0,)), ((), ())), preferred_element_type=F32
    ).astype(BF)
    wide = 2 * half // cols
    deep = slots // wide
    expert_block = (
        expert_rows.reshape(wide, deep, cols).transpose(1, 0, 2).reshape(deep, 2 * half)
    )
    share = total // n_tp
    arrived = exchange(
        jnp.concatenate(
            [dense_partial.reshape(n_tp, share, 2 * half), to_everyone(expert_block, n_tp)],
            axis=1,
        ),
        "tp",
    )
    dense_inner = jnp.sum(arrived[:, :share].astype(F32), axis=0)
    rows = (
        arrived[:, share:]
        .reshape(n_tp, deep, wide, cols)
        .transpose(2, 1, 0, 3)
        .reshape(slots, width)
    )
    plain_rows = rows.astype(F32) / moe_gain
    row_scale = lax.rsqrt(jnp.mean(plain_rows * plain_rows, axis=1, keepdims=True) + EPS)

    def expert_share(which):
        here = slice(which * per_expert, (which + 1) * per_expert)
        gate_vals = dot32(rows[here], gate_pair[which]) * row_scale[here]
        up_vals = dot32(rows[here], up_pair[which]) * row_scale[here]
        act = (jax.nn.silu(gate_vals) * up_vals).astype(BF)
        return dot32(act, down_pair[which]).astype(BF)

    partial_out = jnp.concatenate([expert_share(0), expert_share(1)], axis=0)
    out_pieces = partial_out.reshape(slots, n_tp, cols).transpose(1, 0, 2)
    scale = lax.rsqrt(dense_inner[:, units + 1 : units + 2] / width + EPS)
    blend = jax.nn.sigmoid(dense_inner[:, units : units + 1] * scale)
    dense_act = (
        blend * jax.nn.silu(dense_inner[:, :half] * scale) * (dense_inner[:, half:] * scale)
    ).astype(BF)
    tiles = half // 128
    act_block = dense_act.reshape(share, tiles, 128).transpose(1, 0, 2).reshape(tiles * share, 128)
    arrived = exchange(
        jnp.concatenate([out_pieces, to_everyone(act_block, n_tp)], axis=1), "tp"
    )
    expert_out = jnp.sum(arrived[:, :slots].astype(F32), axis=0) * slot_weight
    act_all = (
        arrived[:, slots:]
        .reshape(n_tp, tiles, share, 128)
        .transpose(0, 2, 1, 3)
        .reshape(total, half)
    )
    down = jnp.pad(chip_down, ((0, half - units), (0, 0)))
    summed = dot32(act_all, down) + dot32(chosen, expert_out.astype(BF))
    final = exchange(summed.astype(BF).reshape(chips, seqs, cols), "ep", same_core)
    output = resid + jnp.sum(final.astype(F32), axis=0)
    return (output, new_recurrent[:, None], inner_window[:, 1:], new_access)


def solution(mesh):
    in_specs = (
        P("ep", None),
        P(),
        P("ep", "tp"),
        P("ep", "tp"),
        P("ep", None),
        P("ep", None),
        P("ep", None),
        P(),
        P(),
        P(),
        P(None, "tp"),
        P(),
        P("ep", None, "tp"),
        P("ep", None, None, None),
        P("ep", "tp", None, None),
        P("tp"),
        P("tp", None),
        P(),
        P("ep", None),
        P("ep", None),
        P("ep", None, "tp"),
        P("ep", None, "tp"),
        P("ep", "tp", None),
        P(),
        P("tp", "ep"),
        P("tp", "ep"),
        P("ep", "tp"),
    )
    out_specs = (
        P("ep", "tp"),
        P("ep", "tp", None, None),
        P("ep", None, "tp"),
        P("ep", None, None, None),
    )
    return jax.shard_map(local, mesh=mesh, in_specs=in_specs, out_specs=out_specs, check_vma=False)
```

```python
import jax
import jax.numpy as jnp
from jax import lax
from jax.sharding import PartitionSpec as P

HEADS = 16
HEAD_DIM = 64
GROUPS = 4
STATE = 128
TOP = 2
PER_GROUP = HEADS // GROUPS
EPS = 1e-06
BF = jnp.bfloat16
F32 = jnp.float32
CORES = 2
CLASSES = 8


def exchange(pieces, axis, groups=None):
    return lax.all_to_all(
        pieces, axis, split_axis=0, concat_axis=0, tiled=True, axis_index_groups=groups
    )


def to_everyone(shard, peers):
    return jnp.broadcast_to(shard[None], (peers, *shard.shape))


def rms_scale(values, gain):
    mean_square = jnp.mean(values * values, axis=-1, keepdims=True)
    return values * lax.rsqrt(mean_square + EPS) * gain


def dot32(left, right):
    return jnp.dot(left, right, preferred_element_type=F32)


def slice_at(array, start, size, dim):
    return lax.dynamic_slice_in_dim(array, start, size, dim)


def local(
    tokens,
    mix_gain,
    gate_weight,
    inner_weight,
    write_weight,
    read_weight,
    step_weight,
    step_bias,
    decay_log,
    skip_scale,
    inner_taps,
    access_taps,
    inner_history,
    access_history,
    recurrent,
    head_gain,
    mixer_out,
    moe_gain,
    expert_ids,
    route_scores,
    expert_gate,
    expert_up,
    expert_down,
    blend_vector,
    dense_gate,
    dense_up,
    dense_down,
):
    seqs, width = tokens.shape
    n_ep = lax.axis_size("ep")
    n_tp = lax.axis_size("tp")
    chips = n_ep // CORES
    ep = lax.axis_index("ep")
    tp = lax.axis_index("tp")
    core = ep % CORES
    group = tp // PER_GROUP
    rows_k = gate_weight.shape[0]
    cols = width // n_tp
    same_core = [[CORES * z + c for z in range(chips)] for c in range(CORES)]

    def from_other_core(shard):
        return lax.ppermute(shard, "ep", [(i, i ^ 1) for i in range(n_ep)])

    per_class = n_ep // CLASSES
    first_class = ep // CLASSES
    near = [[CLASSES * j + r for r in range(CLASSES)] for j in range(per_class)]

    write_own = slice_at(write_weight, group * STATE, STATE, 1)
    read_own = slice_at(read_weight, group * STATE, STATE, 1)
    main = jnp.concatenate([gate_weight, inner_weight, write_own, read_own], axis=1)
    pack_cols = main.shape[1]
    head_pick = (jnp.arange(HEADS) == tp).astype(BF)[None]
    step_row = lax.dot_general(
        head_pick, step_weight, (((1,), (1,)), ((), ())), preferred_element_type=F32
    ).astype(BF)
    first = jax.nn.sigmoid(route_scores[:, 0] - route_scores[:, 1])
    first_high = lax.reduce_precision(first, 8, 7)
    first_low = first - first_high
    lane = jnp.arange(4 * seqs)[None]
    spread = jnp.where(
        lane < seqs,
        expert_ids[:, 0:1].astype(F32),
        jnp.where(
            lane < 2 * seqs,
            expert_ids[:, 1:2].astype(F32),
            jnp.where(lane < 3 * seqs, first_high[:, None], first_low[:, None]),
        ),
    )
    route_row = jnp.sum(
        jnp.where(lane % seqs == jnp.arange(seqs)[:, None], spread, 0.0), axis=0, keepdims=True
    ).astype(BF)
    extra = jnp.concatenate([step_row, route_row, jnp.zeros((6, rows_k), BF)], axis=0)
    extra = jnp.pad(extra, ((0, 0), (0, pack_cols - rows_k)))
    pack = jnp.concatenate([main, extra], axis=0)
    class_pack = [pack]
    for ahead in range(1, per_class):
        hops = [(i, (i - CLASSES * ahead) % n_ep) for i in range(n_ep)]
        class_pack.append(lax.ppermute(pack, "ep", hops))
    class_pack = jnp.stack(class_pack)

    normed = rms_scale(tokens.astype(F32), mix_gain).astype(BF)
    rotated = slice_at(
        jnp.concatenate([normed, normed], axis=1), first_class * CLASSES * rows_k, width, 1
    )
    keys = rotated.reshape(seqs, per_class, CLASSES, rows_k).transpose(2, 0, 1, 3)
    keys = exchange(keys.reshape(CLASSES, seqs, per_class * rows_k), "ep", near)
    keys = keys.reshape(CLASSES * seqs, per_class, rows_k)
    padded = jnp.pad(keys, ((0, 0), (0, 0), (0, pack.shape[0] - rows_k)))
    main_share = dot32(padded.reshape(CLASSES * seqs, -1), class_pack.reshape(-1, pack_cols))
    step_rows = class_pack[:, rows_k, :rows_k].astype(F32)
    step_share = jnp.sum(keys.astype(F32) * step_rows[None], axis=(1, 2)).reshape(CLASSES, seqs, 1)
    route_rows = class_pack[:, rows_k + 1, : 4 * seqs].astype(F32)
    route_rows = jnp.pad(route_rows, ((0, seqs - per_class), (0, 0)))
    outgoing = (
        jnp.concatenate(
            [
                main_share.reshape(CLASSES, seqs, pack_cols),
                step_share,
                jnp.zeros((CLASSES, seqs, 63), F32),
                to_everyone(route_rows, CLASSES),
            ],
            axis=2,
        )
    )
    shares = exchange(outgoing, "ep", near)
    projected = jnp.sum(shares[:, :, : pack_cols + 1], axis=0)
    step_raw = projected[:, pack_cols]
    own_routes = lax.dynamic_index_in_dim(
        shares[:, :per_class, pack_cols + 64 :].reshape(
            CLASSES // CORES, CORES, per_class, 4 * seqs
        ),
        core,
        1,
        False,
    )
    own_routes = own_routes.transpose(1, 0, 2).reshape(chips, 4 * seqs)
    gate_part = projected[:, :HEAD_DIM].astype(BF)
    inner_part = projected[:, HEAD_DIM : 2 * HEAD_DIM].astype(BF)
    write_part = projected[:, 2 * HEAD_DIM : 2 * HEAD_DIM + STATE].astype(BF)
    read_part = projected[:, 2 * HEAD_DIM + STATE : pack_cols].astype(BF)

    inner_window = jnp.concatenate([inner_history, inner_part[:, None, :]], axis=1)
    inner_conv = jax.nn.silu(
        jnp.sum(inner_window.astype(F32) * inner_taps.astype(F32)[None], axis=1)
    )
    history_own = slice_at(access_history, group * STATE, STATE, 3).astype(F32)
    taps_own = slice_at(access_taps, group * STATE, STATE, 2).astype(F32)

    def access_conv(which, part):
        taps = taps_own[which]
        past = jnp.sum(history_own[:, which] * taps[None, :3], axis=1)
        return jax.nn.silu(past + part.astype(F32) * taps[3][None])

    write_conv = access_conv(0, write_part)
    read_conv = access_conv(1, read_part)
    bias_own = slice_at(step_bias, tp, 1, 0)
    rate_own = slice_at(decay_log, tp, 1, 0)
    skip_own = slice_at(skip_scale, tp, 1, 0)
    step = jax.nn.softplus(step_raw + bias_own)
    decay = jnp.exp(-step * jnp.exp(rate_own))
    new_recurrent = (
        decay[:, None, None] * recurrent[:, 0]
        + (step[:, None] * inner_conv)[..., None] * write_conv[:, None, :]
    )
    readout = jnp.sum(new_recurrent * read_conv[:, None, :], axis=-1) + skip_own * inner_conv
    gated = readout * jax.nn.silu(gate_part.astype(F32))
    head_out = rms_scale(gated, head_gain).astype(BF)

    total = chips * seqs
    at = jnp.arange(total)[:, None]
    source = (jnp.arange(chips)[None] + first_class * (CLASSES // CORES)) % chips
    by_source = (at // seqs == source).astype(BF)
    route_rows = dot32(by_source, own_routes.astype(BF))
    route_lane = jnp.arange(4 * seqs)[None]
    class_routes = jnp.concatenate(
        [
            jnp.sum(
                jnp.where(route_lane == which * seqs + at % seqs, route_rows, 0.0),
                axis=1,
                keepdims=True,
            )
            for which in range(4)
        ],
        axis=1,
    )

    units = CORES * dense_gate.shape[1]
    gate_pair = [expert_gate[0], from_other_core(expert_gate[0])]
    up_pair = [expert_up[0], from_other_core(expert_up[0])]
    down_pair = [expert_down[0], from_other_core(expert_down[0])]
    own_dense = jnp.concatenate([dense_gate, dense_up], axis=1)
    other_dense = from_other_core(own_dense)
    chip_down = jnp.concatenate([dense_down, from_other_core(dense_down)], axis=0)

    partial_mix = dot32(head_out, mixer_out)
    mix_pieces = partial_mix.astype(BF).reshape(seqs, n_tp, cols).transpose(1, 0, 2)
    parts_sent = jnp.where(tp % 2 == 0, write_part, read_part)
    arrived = exchange(
        jnp.concatenate([mix_pieces, to_everyone(parts_sent, n_tp)], axis=1), "tp"
    )
    mixed = jnp.sum(arrived[:, :seqs].astype(F32), axis=0).astype(BF)
    parts_all = arrived[:, seqs:].reshape(GROUPS, PER_GROUP, seqs, STATE)[:, :2]
    parts_all = parts_all.transpose(2, 1, 0, 3).reshape(seqs, 2, 1, GROUPS * STATE)
    new_access = jnp.concatenate([access_history[:, :, 1:], parts_all], axis=2)

    resid = slice_at(tokens, tp * cols, cols, 1).astype(F32) + mixed.astype(F32)
    gain_own = slice_at(moe_gain, tp * cols, cols, 0)
    scaled = (resid * gain_own).astype(BF)
    class_scaled = exchange(to_everyone(scaled, chips), "ep", same_core).reshape(total, cols)

    first_all = class_routes[:, 2:3] + class_routes[:, 3:4]
    place = jnp.arange(total)
    block = place // seqs
    earlier = ((block[:, None] == block[None]) & (place[None] < place[:, None])).astype(BF)
    mine = jnp.stack([ep, ep + 1 - 2 * core]).astype(F32)[None]
    is_first = class_routes[:, 0:1] == mine
    named = is_first | (class_routes[:, 1:2] == mine)
    weight = jnp.where(is_first, first_all, 1.0 - first_all)
    weight_high = lax.reduce_precision(weight, 8, 7)
    weight_low = (weight - weight_high).astype(BF)
    rank = jnp.where(named, dot32(earlier, named.astype(BF)), -1.0)
    per_expert = TOP * chips
    slots = CORES * per_expert
    slot = jnp.arange(slots)[None]
    key = jnp.where(slot < per_expert, rank[:, 0:1], rank[:, 1:2])
    chosen = (slot % per_expert // TOP == block[:, None]) & (key == (slot % TOP).astype(F32))
    chosen = chosen.astype(BF)
    by_slot = lax.dot_general(
        chosen,
        jnp.concatenate([weight_high.astype(BF), weight_low], axis=1),
        (((0,), (0,)), ((), ())),
        preferred_element_type=F32,
    )
    slot_weight = jnp.where(
        jnp.arange(slots)[:, None] < per_expert,
        by_slot[:, 0:1] + by_slot[:, 2:3],
        by_slot[:, 1:2] + by_slot[:, 3:4],
    )

    half = -(-(units + 2) // 128) * 128
    own_units = units // CORES
    blend_col = slice_at(blend_vector, tp * cols, cols, 0)[:, None]
    both_dense = jnp.concatenate(
        [
            own_dense[:, :own_units],
            other_dense[:, :own_units],
            blend_col,
            jnp.zeros((cols, half - units - 1), BF),
            own_dense[:, own_units:],
            other_dense[:, own_units:],
            jnp.zeros((cols, half - units), BF),
        ],
        axis=1,
    )
    plain = class_scaled.astype(F32) / gain_own
    square_sum = jnp.sum(plain * plain, axis=1, keepdims=True)
    dense_partial = dot32(class_scaled, both_dense)
    dense_partial = jnp.where(
        jnp.arange(2 * half)[None] == units + 1, square_sum, dense_partial
    ).astype(BF)
    expert_rows = lax.dot_general(
        chosen, class_scaled, (((0,), (0,)), ((), ())), preferred_element_type=F32
    ).astype(BF)
    wide = 2 * half // cols
    deep = slots // wide
    expert_block = (
        expert_rows.reshape(wide, deep, cols).transpose(1, 0, 2).reshape(deep, 2 * half)
    )
    share = total // n_tp
    arrived = exchange(
        jnp.concatenate(
            [dense_partial.reshape(n_tp, share, 2 * half), to_everyone(expert_block, n_tp)],
            axis=1,
        ),
        "tp",
    )
    dense_inner = jnp.sum(arrived[:, :share].astype(F32), axis=0)
    rows = (
        arrived[:, share:]
        .reshape(n_tp, deep, wide, cols)
        .transpose(2, 1, 0, 3)
        .reshape(slots, width)
    )
    plain_rows = rows.astype(F32) / moe_gain
    row_scale = lax.rsqrt(jnp.mean(plain_rows * plain_rows, axis=1, keepdims=True) + EPS)

    def expert_share(which):
        here = slice(which * per_expert, (which + 1) * per_expert)
        gate_vals = dot32(rows[here], gate_pair[which]) * row_scale[here]
        up_vals = dot32(rows[here], up_pair[which]) * row_scale[here]
        act = (jax.nn.silu(gate_vals) * up_vals).astype(BF)
        return dot32(act, down_pair[which]).astype(BF)

    partial_out = jnp.concatenate([expert_share(0), expert_share(1)], axis=0)
    out_pieces = partial_out.reshape(slots, n_tp, cols).transpose(1, 0, 2)
    scale = lax.rsqrt(dense_inner[:, units + 1 : units + 2] / width + EPS)
    blend = jax.nn.sigmoid(dense_inner[:, units : units + 1] * scale)
    dense_act = (
        blend * jax.nn.silu(dense_inner[:, :half] * scale) * (dense_inner[:, half:] * scale)
    ).astype(BF)
    tiles = half // 128
    act_block = dense_act.reshape(share, tiles, 128).transpose(1, 0, 2).reshape(tiles * share, 128)
    arrived = exchange(
        jnp.concatenate([out_pieces, to_everyone(act_block, n_tp)], axis=1), "tp"
    )
    expert_out = jnp.sum(arrived[:, :slots].astype(F32), axis=0) * slot_weight
    act_all = (
        arrived[:, slots:]
        .reshape(n_tp, tiles, share, 128)
        .transpose(0, 2, 1, 3)
        .reshape(total, half)
    )
    down = jnp.pad(chip_down, ((0, half - units), (0, 0)))
    summed = dot32(act_all, down) + dot32(chosen, expert_out.astype(BF))
    final = exchange(summed.astype(BF).reshape(chips, seqs, cols), "ep", same_core)
    output = resid + jnp.sum(final.astype(F32), axis=0)
    return (output, new_recurrent[:, None], inner_window[:, 1:], new_access)


def solution(mesh):
    in_specs = (
        P("ep", None),
        P(),
        P("ep", "tp"),
        P("ep", "tp"),
        P("ep", None),
        P("ep", None),
        P("ep", None),
        P(),
        P(),
        P(),
        P(None, "tp"),
        P(),
        P("ep", None, "tp"),
        P("ep", None, None, None),
        P("ep", "tp", None, None),
        P("tp"),
        P("tp", None),
        P(),
        P("ep", None),
        P("ep", None),
        P("ep", None, "tp"),
        P("ep", None, "tp"),
        P("ep", "tp", None),
        P(),
        P("tp", "ep"),
        P("tp", "ep"),
        P("ep", "tp"),
    )
    out_specs = (
        P("ep", "tp"),
        P("ep", "tp", None, None),
        P("ep", None, "tp"),
        P("ep", None, None, None),
    )
    return jax.shard_map(
        local, mesh=mesh, in_specs=in_specs, out_specs=out_specs, check_vma=False
    )
```

```python
import jax
import jax.numpy as jnp
from jax import lax
from jax.sharding import PartitionSpec as P

HEADS = 16
HEAD_DIM = 64
GROUPS = 4
STATE = 128
TOP = 2
PER_GROUP = HEADS // GROUPS
EPS = 1e-06
BF = jnp.bfloat16
F32 = jnp.float32
CORES = 2
CLASSES = 8


def exchange(pieces, axis, groups=None):
    return lax.all_to_all(
        pieces, axis, split_axis=0, concat_axis=0, tiled=True, axis_index_groups=groups
    )


def to_everyone(shard, peers):
    return jnp.broadcast_to(shard[None], (peers, *shard.shape))


def rms_scale(values, gain):
    mean_square = jnp.mean(values * values, axis=-1, keepdims=True)
    return values * lax.rsqrt(mean_square + EPS) * gain


def dot32(left, right):
    return jnp.dot(left, right, preferred_element_type=F32)


def slice_at(array, start, size, dim):
    return lax.dynamic_slice_in_dim(array, start, size, dim)


def local(
    tokens,
    mix_gain,
    gate_weight,
    inner_weight,
    write_weight,
    read_weight,
    step_weight,
    step_bias,
    decay_log,
    skip_scale,
    inner_taps,
    access_taps,
    inner_history,
    access_history,
    recurrent,
    head_gain,
    mixer_out,
    moe_gain,
    expert_ids,
    route_scores,
    expert_gate,
    expert_up,
    expert_down,
    blend_vector,
    dense_gate,
    dense_up,
    dense_down,
):
    seqs, width = tokens.shape
    n_ep = lax.axis_size("ep")
    n_tp = lax.axis_size("tp")
    chips = n_ep // CORES
    ep = lax.axis_index("ep")
    tp = lax.axis_index("tp")
    core = ep % CORES
    group = tp // PER_GROUP
    rows_k = gate_weight.shape[0]
    cols = width // n_tp
    same_core = [[CORES * z + c for z in range(chips)] for c in range(CORES)]

    def from_other_core(shard):
        return lax.ppermute(shard, "ep", [(i, i ^ 1) for i in range(n_ep)])

    per_class = n_ep // CLASSES
    first_class = ep // CLASSES
    near = [[CLASSES * j + r for r in range(CLASSES)] for j in range(per_class)]

    write_own = slice_at(write_weight, group * STATE, STATE, 1)
    read_own = slice_at(read_weight, group * STATE, STATE, 1)
    main = jnp.concatenate([gate_weight, inner_weight, write_own, read_own], axis=1)
    pack_cols = main.shape[1]
    head_pick = (jnp.arange(HEADS) == tp).astype(BF)[None]
    step_row = lax.dot_general(
        head_pick, step_weight, (((1,), (1,)), ((), ())), preferred_element_type=F32
    ).astype(BF)
    first = jax.nn.sigmoid(route_scores[:, 0] - route_scores[:, 1])
    first_high = lax.reduce_precision(first, 8, 7)
    first_low = first - first_high
    lane = jnp.arange(4 * seqs)[None]
    spread = jnp.where(
        lane < seqs,
        expert_ids[:, 0:1].astype(F32),
        jnp.where(
            lane < 2 * seqs,
            expert_ids[:, 1:2].astype(F32),
            jnp.where(lane < 3 * seqs, first_high[:, None], first_low[:, None]),
        ),
    )
    route_row = jnp.sum(
        jnp.where(lane % seqs == jnp.arange(seqs)[:, None], spread, 0.0), axis=0, keepdims=True
    ).astype(BF)
    extra = jnp.concatenate([step_row, route_row, jnp.zeros((6, rows_k), BF)], axis=0)
    extra = jnp.pad(extra, ((0, 0), (0, pack_cols - rows_k)))
    pack = jnp.concatenate([main, extra], axis=0)
    def from_ahead(shard, classes_on):
        hops = [(i, (i - CLASSES * classes_on) % n_ep) for i in range(n_ep)]
        return lax.ppermute(shard, "ep", hops)

    class_pack = [pack, from_ahead(pack, 1)]
    for ahead in range(2, per_class - 1):
        class_pack.append(from_ahead(class_pack[-1], 1))
    class_pack.append(from_ahead(pack, -1))
    class_pack = jnp.stack(class_pack)

    normed = rms_scale(tokens.astype(F32), mix_gain).astype(BF)
    rotated = slice_at(
        jnp.concatenate([normed, normed], axis=1), first_class * CLASSES * rows_k, width, 1
    )
    keys = rotated.reshape(seqs, per_class, CLASSES, rows_k).transpose(2, 0, 1, 3)
    keys = exchange(keys.reshape(CLASSES, seqs, per_class * rows_k), "ep", near)
    keys = keys.reshape(CLASSES * seqs, per_class, rows_k)
    padded = jnp.pad(keys, ((0, 0), (0, 0), (0, pack.shape[0] - rows_k)))
    main_share = dot32(padded.reshape(CLASSES * seqs, -1), class_pack.reshape(-1, pack_cols))
    step_rows = class_pack[:, rows_k, :rows_k].astype(F32)
    step_share = jnp.sum(keys.astype(F32) * step_rows[None], axis=(1, 2)).reshape(CLASSES, seqs, 1)
    route_rows = class_pack[:, rows_k + 1, : 4 * seqs].astype(F32)
    route_rows = jnp.pad(route_rows, ((0, seqs - per_class), (0, 0)))
    shares = exchange(
        jnp.concatenate(
            [
                main_share.reshape(CLASSES, seqs, pack_cols),
                step_share,
                jnp.zeros((CLASSES, seqs, 63), F32),
                to_everyone(route_rows, CLASSES),
            ],
            axis=2,
        ),
        "ep",
        near,
    )
    projected = jnp.sum(shares[:, :, : pack_cols + 1], axis=0)
    step_raw = projected[:, pack_cols]
    own_routes = lax.dynamic_index_in_dim(
        shares[:, :per_class, pack_cols + 64 :].reshape(
            CLASSES // CORES, CORES, per_class, 4 * seqs
        ),
        core,
        1,
        False,
    )
    own_routes = own_routes.transpose(1, 0, 2).reshape(chips, 4 * seqs)
    gate_part = projected[:, :HEAD_DIM].astype(BF)
    inner_part = projected[:, HEAD_DIM : 2 * HEAD_DIM].astype(BF)
    write_part = projected[:, 2 * HEAD_DIM : 2 * HEAD_DIM + STATE].astype(BF)
    read_part = projected[:, 2 * HEAD_DIM + STATE : pack_cols].astype(BF)

    inner_window = jnp.concatenate([inner_history, inner_part[:, None, :]], axis=1)
    inner_conv = jax.nn.silu(
        jnp.sum(inner_window.astype(F32) * inner_taps.astype(F32)[None], axis=1)
    )
    history_own = slice_at(access_history, group * STATE, STATE, 3).astype(F32)
    taps_own = slice_at(access_taps, group * STATE, STATE, 2).astype(F32)

    def access_conv(which, part):
        taps = taps_own[which]
        past = jnp.sum(history_own[:, which] * taps[None, :3], axis=1)
        return jax.nn.silu(past + part.astype(F32) * taps[3][None])

    write_conv = access_conv(0, write_part)
    read_conv = access_conv(1, read_part)
    bias_own = slice_at(step_bias, tp, 1, 0)
    rate_own = slice_at(decay_log, tp, 1, 0)
    skip_own = slice_at(skip_scale, tp, 1, 0)
    step = jax.nn.softplus(step_raw + bias_own)
    decay = jnp.exp(-step * jnp.exp(rate_own))
    new_recurrent = (
        decay[:, None, None] * recurrent[:, 0]
        + (step[:, None] * inner_conv)[..., None] * write_conv[:, None, :]
    )
    readout = jnp.sum(new_recurrent * read_conv[:, None, :], axis=-1) + skip_own * inner_conv
    gated = readout * jax.nn.silu(gate_part.astype(F32))
    head_out = rms_scale(gated, head_gain).astype(BF)

    total = chips * seqs
    at = jnp.arange(total)[:, None]
    source = (jnp.arange(chips)[None] + first_class * (CLASSES // CORES)) % chips
    by_source = (at // seqs == source).astype(BF)
    route_rows = dot32(by_source, own_routes.astype(BF))
    route_lane = jnp.arange(4 * seqs)[None]
    class_routes = jnp.concatenate(
        [
            jnp.sum(
                jnp.where(route_lane == which * seqs + at % seqs, route_rows, 0.0),
                axis=1,
                keepdims=True,
            )
            for which in range(4)
        ],
        axis=1,
    )

    units = CORES * dense_gate.shape[1]
    gate_pair = [expert_gate[0], from_other_core(expert_gate[0])]
    up_pair = [expert_up[0], from_other_core(expert_up[0])]
    down_pair = [expert_down[0], from_other_core(expert_down[0])]
    own_dense = jnp.concatenate([dense_gate, dense_up], axis=1)
    other_dense = from_other_core(own_dense)
    chip_down = jnp.concatenate([dense_down, from_other_core(dense_down)], axis=0)

    partial_mix = dot32(head_out, mixer_out)
    mix_pieces = partial_mix.astype(BF).reshape(seqs, n_tp, cols).transpose(1, 0, 2)
    parts_sent = jnp.where(tp % 2 == 0, write_part, read_part)
    arrived = exchange(
        jnp.concatenate([mix_pieces, to_everyone(parts_sent, n_tp)], axis=1), "tp"
    )
    mixed = jnp.sum(arrived[:, :seqs].astype(F32), axis=0).astype(BF)
    parts_all = arrived[:, seqs:].reshape(GROUPS, PER_GROUP, seqs, STATE)[:, :2]
    parts_all = parts_all.transpose(2, 1, 0, 3).reshape(seqs, 2, 1, GROUPS * STATE)
    new_access = jnp.concatenate([access_history[:, :, 1:], parts_all], axis=2)

    resid = slice_at(tokens, tp * cols, cols, 1).astype(F32) + mixed.astype(F32)
    gain_own = slice_at(moe_gain, tp * cols, cols, 0)
    scaled = (resid * gain_own).astype(BF)
    class_scaled = exchange(to_everyone(scaled, chips), "ep", same_core).reshape(total, cols)

    first_all = class_routes[:, 2:3] + class_routes[:, 3:4]
    place = jnp.arange(total)
    block = place // seqs
    earlier = ((block[:, None] == block[None]) & (place[None] < place[:, None])).astype(BF)
    mine = jnp.stack([ep, ep + 1 - 2 * core]).astype(F32)[None]
    is_first = class_routes[:, 0:1] == mine
    named = is_first | (class_routes[:, 1:2] == mine)
    weight = jnp.where(is_first, first_all, 1.0 - first_all)
    weight_high = lax.reduce_precision(weight, 8, 7)
    weight_low = (weight - weight_high).astype(BF)
    rank = jnp.where(named, dot32(earlier, named.astype(BF)), -1.0)
    per_expert = TOP * chips
    slots = CORES * per_expert
    slot = jnp.arange(slots)[None]
    key = jnp.where(slot < per_expert, rank[:, 0:1], rank[:, 1:2])
    chosen = (slot % per_expert // TOP == block[:, None]) & (key == (slot % TOP).astype(F32))
    chosen = chosen.astype(BF)
    by_slot = lax.dot_general(
        chosen,
        jnp.concatenate([weight_high.astype(BF), weight_low], axis=1),
        (((0,), (0,)), ((), ())),
        preferred_element_type=F32,
    )
    slot_weight = jnp.where(
        jnp.arange(slots)[:, None] < per_expert,
        by_slot[:, 0:1] + by_slot[:, 2:3],
        by_slot[:, 1:2] + by_slot[:, 3:4],
    )

    half = -(-(units + 2) // 128) * 128
    own_units = units // CORES
    blend_col = slice_at(blend_vector, tp * cols, cols, 0)[:, None]
    both_dense = jnp.concatenate(
        [
            own_dense[:, :own_units],
            other_dense[:, :own_units],
            blend_col,
            jnp.zeros((cols, half - units - 1), BF),
            own_dense[:, own_units:],
            other_dense[:, own_units:],
            jnp.zeros((cols, half - units), BF),
        ],
        axis=1,
    )
    plain = class_scaled.astype(F32) / gain_own
    square_sum = jnp.sum(plain * plain, axis=1, keepdims=True)
    dense_partial = dot32(class_scaled, both_dense)
    dense_partial = jnp.where(
        jnp.arange(2 * half)[None] == units + 1, square_sum, dense_partial
    ).astype(BF)
    expert_rows = lax.dot_general(
        chosen, class_scaled, (((0,), (0,)), ((), ())), preferred_element_type=F32
    ).astype(BF)
    wide = 2 * half // cols
    deep = slots // wide
    expert_block = (
        expert_rows.reshape(wide, deep, cols).transpose(1, 0, 2).reshape(deep, 2 * half)
    )
    share = total // n_tp
    arrived = exchange(
        jnp.concatenate(
            [dense_partial.reshape(n_tp, share, 2 * half), to_everyone(expert_block, n_tp)],
            axis=1,
        ),
        "tp",
    )
    dense_inner = jnp.sum(arrived[:, :share].astype(F32), axis=0)
    rows = (
        arrived[:, share:]
        .reshape(n_tp, deep, wide, cols)
        .transpose(2, 1, 0, 3)
        .reshape(slots, width)
    )
    plain_rows = rows.astype(F32) / moe_gain
    row_scale = lax.rsqrt(jnp.mean(plain_rows * plain_rows, axis=1, keepdims=True) + EPS)

    def expert_share(which):
        here = slice(which * per_expert, (which + 1) * per_expert)
        gate_vals = dot32(rows[here], gate_pair[which]) * row_scale[here]
        up_vals = dot32(rows[here], up_pair[which]) * row_scale[here]
        act = (jax.nn.silu(gate_vals) * up_vals).astype(BF)
        return dot32(act, down_pair[which]).astype(BF)

    partial_out = jnp.concatenate([expert_share(0), expert_share(1)], axis=0)
    out_pieces = partial_out.reshape(slots, n_tp, cols).transpose(1, 0, 2)
    scale = lax.rsqrt(dense_inner[:, units + 1 : units + 2] / width + EPS)
    blend = jax.nn.sigmoid(dense_inner[:, units : units + 1] * scale)
    dense_act = (
        blend * jax.nn.silu(dense_inner[:, :half] * scale) * (dense_inner[:, half:] * scale)
    ).astype(BF)
    tiles = half // 128
    act_block = dense_act.reshape(share, tiles, 128).transpose(1, 0, 2).reshape(tiles * share, 128)
    arrived = exchange(
        jnp.concatenate([out_pieces, to_everyone(act_block, n_tp)], axis=1), "tp"
    )
    expert_out = jnp.sum(arrived[:, :slots].astype(F32), axis=0) * slot_weight
    act_all = (
        arrived[:, slots:]
        .reshape(n_tp, tiles, share, 128)
        .transpose(0, 2, 1, 3)
        .reshape(total, half)
    )
    down = jnp.pad(chip_down, ((0, half - units), (0, 0)))
    summed = dot32(act_all, down) + dot32(chosen, expert_out.astype(BF))
    final = exchange(summed.astype(BF).reshape(chips, seqs, cols), "ep", same_core)
    output = resid + jnp.sum(final.astype(F32), axis=0)
    return (output, new_recurrent[:, None], inner_window[:, 1:], new_access)


def solution(mesh):
    in_specs = (
        P("ep", None),
        P(),
        P("ep", "tp"),
        P("ep", "tp"),
        P("ep", None),
        P("ep", None),
        P("ep", None),
        P(),
        P(),
        P(),
        P(None, "tp"),
        P(),
        P("ep", None, "tp"),
        P("ep", None, None, None),
        P("ep", "tp", None, None),
        P("tp"),
        P("tp", None),
        P(),
        P("ep", None),
        P("ep", None),
        P("ep", None, "tp"),
        P("ep", None, "tp"),
        P("ep", "tp", None),
        P(),
        P("tp", "ep"),
        P("tp", "ep"),
        P("ep", "tp"),
    )
    out_specs = (
        P("ep", "tp"),
        P("ep", "tp", None, None),
        P("ep", None, "tp"),
        P("ep", None, None, None),
    )
    return jax.shard_map(local, mesh=mesh, in_specs=in_specs, out_specs=out_specs, check_vma=False)
```
